32 devices in a mesh: sp: 8 (over z, x), tp: 4 (over y, core).
Axes of the slice: x: 2, y: 2, z: 4, core: 2. Of those that a mesh axis runs over, the one named last changes fastest.
Arguments:
- latent: bfloat16 [4096, 2048], P('sp'), may hold values from -6 to 6
- context: bfloat16 [512, 2048], P('sp'), may hold values from -6 to 6
- condition: bfloat16 [2048], replicated, may hold values from -6 to 6
- context_condition: bfloat16 [2048], replicated, may hold values from -6 to 6
- shift_weight: bfloat16 [2048, 2048], P('sp', 'tp'), may hold values from -0.125 to 0.125
- scale_weight: bfloat16 [2048, 2048], P('sp', 'tp'), may hold values from -0.125 to 0.125
- mod_gate_weight: bfloat16 [2048, 2048], P('sp', 'tp'), may hold values from -0.5 to 0.5
- norm_gain: bfloat16 [2048], replicated, may hold values from 0.099609375 to 1.8984375
- query_weight: bfloat16 [2048, 2048], P(None, 'tp'), may hold values from -0.125 to 0.125
- key_weight: bfloat16 [2048, 2048], P(None, 'tp'), may hold values from -0.125 to 0.125
- value_weight: bfloat16 [2048, 2048], P(None, 'tp'), may hold values from -0.125 to 0.125
- gate_weight: bfloat16 [2048, 2048], P(None, 'tp'), may hold values from -0.125 to 0.125
- forward_decay: float32 [16], P('tp'), may hold values from 0 to 1, as said below
- backward_decay: float32 [16], P('tp'), may hold values from 0 to 1, as said below
- out_weight: bfloat16 [2048, 2048], P('tp'), may hold values from -0.125 to 0.125
Outputs:
- mixed: bfloat16 [4096, 2048], P('sp')
The draws below stay inside these ranges and needn't reach their ends.
Inputs may be any that keep to these rules, and one draw needn't show every extreme that they name: `forward_decay`: each head's rate is positive. `backward_decay`: each head's rate is positive.
All inputs are finite; a program needn't handle non-finite values.
Results may differ from the reference program's by a relative error of at most 0.015.
Values may be sent and summed in bfloat16 or wider, within the bound.
A program may use at most 64 MiB of HBM per device.

```python
import jax
import jax.numpy as jnp
from jax import lax

D = 2048
HEAD_DIM = 128
RET_HEADS = 16
RET_WIDTH = 2048
GRID_W = 64
SEQ = 4096
CTX = 512


def decay_rates(key, fast_share):
    pick_key, fast_key, slow_key = jax.random.split(key, 3)
    fast = jax.random.uniform(pick_key, (RET_HEADS,), jnp.float32) < fast_share
    fast_rate = jnp.exp(jax.random.uniform(fast_key, (RET_HEADS,), jnp.float32, jnp.log(1.0 / 100.0), jnp.log(1.0 / 30.0)))
    slow_rate = jnp.exp(jax.random.uniform(slow_key, (RET_HEADS,), jnp.float32, jnp.log(0.2), jnp.log(2.0))) / SEQ
    return jnp.where(fast, fast_rate, slow_rate).astype(jnp.float32)


def draw_forward_decay(key, part):
    share = 0.5
    return decay_rates(jax.random.fold_in(key, 11), share)


def draw_backward_decay(key, part):
    share = 0.5
    return decay_rates(jax.random.fold_in(key, 23), share)


def level_of(key, extent, cuts, smallest, top_value):
    loudness = 1.0
    for position, blocks in cuts:
        heights = jax.random.uniform(jax.random.fold_in(jax.random.fold_in(key, 6), position), (blocks,), jnp.float32, smallest / len(cuts), top_value / len(cuts))
        loudness = loudness * jnp.repeat(jnp.exp(heights), extent[position] // blocks).reshape((-1,) + (1,) * (len(extent) - 1 - position))
    return loudness


def noise(key, shape, scale, bound, cuts=(), kind=jnp.bfloat16):
    drawn = jax.random.normal(key, shape, jnp.float32) * scale
    if len(cuts) > 0:
        drawn = level_of(key, shape, cuts, -0.22, 0.18) * drawn
    return jnp.clip(drawn, min=-bound, max=bound).astype(kind)


def setup_inputs(seed: int = 0) -> dict:
    streams_of = jax.random.split(jax.random.key(seed), 16)
    latent = noise(streams_of[0], (SEQ, D), 1.0, 6.0, ((0, 8),))
    context = noise(streams_of[1], (CTX, D), 1.0, 6.0, ((0, 8),))
    condition = noise(streams_of[2], (D,), 1.0, 6.0)
    context_condition = noise(streams_of[3], (D,), 1.0, 6.0)
    shift_weight = noise(streams_of[4], (D, D), D ** -0.5, 0.125, ((0, 8), (1, 4)))
    scale_weight = noise(streams_of[5], (D, D), D ** -0.5, 0.125, ((0, 8), (1, 4)))
    mod_gate_weight = noise(streams_of[6], (D, D), (D // 16) ** -0.5, 0.5, ((0, 8), (1, 4)))
    norm_gain = jnp.clip(1.0 + 0.18 * jax.random.normal(streams_of[7], (D,), jnp.float32), 0.099609375, 1.8984375).astype(jnp.bfloat16)
    query_weight = noise(streams_of[8], (D, RET_WIDTH), D ** -0.5, 0.125, ((1, 4),))
    key_weight = noise(streams_of[9], (D, RET_WIDTH), D ** -0.5, 0.125, ((1, 4),))
    value_weight = noise(streams_of[10], (D, RET_WIDTH), D ** -0.5, 0.125, ((1, 4),))
    gate_weight = noise(streams_of[11], (D, RET_WIDTH), D ** -0.5, 0.125, ((1, 4),))
    forward_decay = draw_forward_decay(jax.random.fold_in(streams_of[15], 71), 0)
    backward_decay = draw_backward_decay(jax.random.fold_in(streams_of[15], 71), 0)
    out_weight = noise(streams_of[14], (RET_WIDTH, D), RET_WIDTH ** -0.5, 0.125, ((0, 4),))
    return dict(latent=latent, context=context, condition=condition, context_condition=context_condition, shift_weight=shift_weight, scale_weight=scale_weight, mod_gate_weight=mod_gate_weight, norm_gain=norm_gain, query_weight=query_weight, key_weight=key_weight, value_weight=value_weight, gate_weight=gate_weight, forward_decay=forward_decay, backward_decay=backward_decay, out_weight=out_weight)


EPS = 1e-06
THETA = 10000.0
CONTEXT_LIFT = 3.0
TOP_PRECISION = lax.Precision.HIGHEST

def modulated(token_rows, norm_gain, shifts, scales):
    values = token_rows.astype(jnp.float32)
    values = values * lax.rsqrt(lax.optimization_barrier(jnp.mean(values * values, axis=-1, keepdims=True)) + EPS)
    values = values * norm_gain.astype(jnp.float32)
    return (values * (1.0 + scales) + shifts).astype(jnp.bfloat16)

def rope_half(portion, positions):
    quarter = portion.shape[-1] // 2
    frequency = THETA ** (-jnp.arange(quarter, dtype=jnp.float32) / quarter)
    angles = positions[:, None, None] * frequency
    cosine = jnp.cos(angles)
    sine_table = jnp.sin(angles)
    leading = portion[..., :quarter]
    trailing = portion[..., quarter:]
    return jnp.concatenate([leading * cosine - trailing * sine_table, leading * sine_table + trailing * cosine], axis=-1)

def rotate(values, grid_row, grid_column):
    half_width = values.shape[-1] // 2
    return jnp.concatenate([rope_half(values[..., :half_width], grid_row), rope_half(values[..., half_width:], grid_column)], axis=-1)

def blockwise(query_heads, key_heads, value_heads, log_decay, initial):
    head_count, length, head_width = query_heads.shape
    block_rows = 128
    block_count = length // block_rows

    def to_blocks(values):
        return jnp.moveaxis(values.reshape(head_count, block_count, block_rows, head_width), 1, 0)
    offsets = jnp.arange(block_rows, dtype=jnp.float32)
    distance = offsets[:, None] - offsets[None, :]
    within_block_decay = jnp.where(distance >= 0, jnp.exp(log_decay[:, None, None] * jnp.maximum(distance, 0.0)), 0.0)
    query_decay = jnp.exp(log_decay[:, None] * (offsets + 1.0))[:, :, None]
    key_decay_factor = jnp.exp(log_decay[:, None] * (block_rows - 1.0 - offsets))[:, :, None]
    per_step_decay = jnp.exp(log_decay * block_rows)[:, None, None]

    def advance(carried_state, pieces):
        query_tile_rows, key_tile_rows, value_tile_rows = pieces
        score_matrix = jnp.einsum('fya,fqa->fyq', query_tile_rows, key_tile_rows, precision=TOP_PRECISION) * within_block_decay
        result_output = jnp.einsum('rij,rjy->riy', score_matrix, value_tile_rows, precision=TOP_PRECISION)
        result_output = result_output + jnp.einsum('hnd,hde->hne', query_tile_rows, carried_state, precision=TOP_PRECISION) * query_decay
        carried_state = carried_state * per_step_decay + jnp.einsum('cwz,cwu->czu', key_tile_rows * key_decay_factor, value_tile_rows, precision=TOP_PRECISION)
        return (carried_state, result_output)
    _, outputs = lax.scan(advance, initial, (to_blocks(query_heads), to_blocks(key_heads), to_blocks(value_heads)))
    return jnp.moveaxis(outputs, 0, 1).reshape(head_count, length, head_width)

def reference(latent, context, condition, context_condition, shift_weight, scale_weight, mod_gate_weight, norm_gain, query_weight, key_weight, value_weight, gate_weight, forward_decay, backward_decay, out_weight):
    activation = jax.nn.silu(jnp.stack([condition, context_condition]).astype(jnp.float32)).astype(jnp.bfloat16)
    shifts = jnp.dot(activation, shift_weight, preferred_element_type=jnp.float32)
    scales = jnp.dot(activation, scale_weight, preferred_element_type=jnp.float32)
    gates = jnp.dot(activation, mod_gate_weight, preferred_element_type=jnp.float32)
    hidden = modulated(latent, norm_gain, shifts[0], scales[0])
    context_hidden = modulated(context, norm_gain, shifts[1], scales[1])
    queries = jnp.dot(hidden, query_weight, preferred_element_type=jnp.float32).astype(jnp.bfloat16)
    keys_out = jnp.dot(hidden, key_weight, preferred_element_type=jnp.float32).astype(jnp.bfloat16)
    values_out = jnp.dot(hidden, value_weight, preferred_element_type=jnp.float32).astype(jnp.bfloat16)
    out_gates = jnp.dot(hidden, gate_weight, preferred_element_type=jnp.float32).astype(jnp.bfloat16)
    context_keys = jnp.dot(context_hidden, key_weight, preferred_element_type=jnp.float32).astype(jnp.bfloat16)
    context_values = jnp.dot(context_hidden, value_weight, preferred_element_type=jnp.float32).astype(jnp.bfloat16)
    length = latent.shape[0]
    positions = jnp.arange(length, dtype=jnp.int32)
    grid_row = (positions // GRID_W).astype(jnp.float32)
    grid_column = (positions % GRID_W).astype(jnp.float32)
    key_scale = HEAD_DIM ** (-0.5)

    def to_heads(values):
        return values.astype(jnp.float32).reshape(values.shape[0], RET_HEADS, HEAD_DIM)
    query_heads = jnp.transpose(rotate(to_heads(queries), grid_row, grid_column), (1, 0, 2))
    key_heads = jnp.transpose(rotate(to_heads(keys_out), grid_row, grid_column), (1, 0, 2)) * key_scale
    value_heads = jnp.transpose(to_heads(values_out), (1, 0, 2))
    log_forward = -forward_decay.astype(jnp.float32)
    log_backward = -backward_decay.astype(jnp.float32)
    context_index = jnp.arange(CTX, dtype=jnp.float32)
    weight_forward = jnp.exp(log_forward[:, None] * (CTX - 1.0 - context_index)[None, :])
    weight_backward = jnp.exp(log_backward[:, None] * context_index[None, :])
    context_key_heads = to_heads(context_keys) * (key_scale * CONTEXT_LIFT)
    context_value_heads = to_heads(context_values)
    context_forward = jnp.einsum('hc,chd,che->hde', weight_forward, context_key_heads, context_value_heads, precision=TOP_PRECISION)
    context_backward = jnp.einsum('hc,chd,che->hde', weight_backward, context_key_heads, context_value_heads, precision=TOP_PRECISION)
    forward_out = blockwise(query_heads, key_heads, value_heads, log_forward, context_forward)
    backward_out = blockwise(jnp.flip(query_heads, 1), jnp.flip(key_heads, 1), jnp.flip(value_heads, 1), log_backward, context_backward)
    retained = forward_out + jnp.flip(backward_out, 1)
    retained = retained * lax.rsqrt(lax.optimization_barrier(jnp.mean(retained * retained, axis=-1, keepdims=True)) + EPS)
    merged = jnp.transpose(retained, (1, 0, 2)).reshape(length, RET_HEADS * HEAD_DIM)
    heads_out = (jax.nn.silu(out_gates.astype(jnp.float32)) * merged).astype(jnp.bfloat16)
    projection = jnp.dot(heads_out, out_weight, preferred_element_type=jnp.float32)
    return (latent.astype(jnp.float32) + gates[0] * projection).astype(jnp.bfloat16)
```

```python
import functools
import math

import jax
import jax.numpy as jnp
from jax import lax
from jax.experimental import pallas as pl
from jax.experimental.pallas import tpu as pltpu
from jax.sharding import PartitionSpec as P

HEAD_DIM = 128
GRID_W = 64
EPS = 1e-06
THETA = 10000.0
CONTEXT_LIFT = 3.0
MESH = pl.DeviceIdType.MESH
F32 = jnp.float32
BF16 = jnp.bfloat16


def dot(a, b):
    return jnp.dot(a, b, preferred_element_type=F32)


def dot_rows(a, b):
    return lax.dot_general(a, b, (((0,), (0,)), ((), ())), preferred_element_type=F32)


def dot_columns(a, b):
    return lax.dot_general(a, b, (((1,), (1,)), ((), ())), preferred_element_type=F32)


def rotated(x, cosines, sines, low):
    partner = jnp.where(low, pltpu.roll(x, HEAD_DIM - 32, 1), pltpu.roll(x, 32, 1))
    return x * cosines + partner * sines


def kernel(
    sp_n,
    tp_n,
    act,
    gain,
    fd,
    bd,
    latent_h,
    context_h,
    shift_h,
    scale_h,
    gate_h,
    wq_h,
    wk_h,
    wv_h,
    wg_h,
    ow_h,
    out_h,
    lat,
    ctx,
    modw,
    wbuf,
    hid,
    mod_part,
    mod_recv,
    mod_sum,
    mod_all,
    inv,
    cosb,
    sinb,
    proj,
    mix,
    local,
    heads_all,
    ow_all,
    acc,
    out_v,
    sc_send,
    sc_recv,
    sl_send,
    sl_recv,
    in_send,
    in_recv,
    load_sem,
    m1s,
    m1r,
    m2s,
    m2r,
    scs,
    scr,
    sls,
    slr,
    ins,
    inr,
    wys,
    wyr,
    wps,
    wpr,
    hys,
    hyr,
    hps,
    hpr,
    out_sem,
):
    me = lax.axis_index("sp")
    tp = lax.axis_index("tp")
    y_n = tp_n // 2
    my_y = tp // 2
    core = lax.rem(tp, 2)
    other = my_y * 2 + 1 - core
    T, D = lat.shape
    CR = ctx.shape[0]
    W = wbuf.shape[2]
    H = W // HEAD_DIM
    R = sl_send.shape[1]
    per = HEAD_DIM // R

    loads = [
        pltpu.make_async_copy(src, dst, load_sem.at[i])
        for i, (src, dst) in enumerate(
            [
                (shift_h, modw.at[0]),
                (scale_h, modw.at[1]),
                (gate_h, modw.at[2]),
                (latent_h, lat),
                (context_h, ctx),
                (wk_h, wbuf.at[1]),
                (wv_h, wbuf.at[2]),
                (wq_h, wbuf.at[0]),
                (wg_h, wbuf.at[3]),
                (ow_h, ow_all.at[pl.ds(tp * H, H)]),
            ]
        )
    ]
    for load in loads:
        load.start()

    barrier = pltpu.get_barrier_semaphore()

    def greet(axis, mine, n):
        def one(off, carry):
            pl.semaphore_signal(
                barrier, inc=1, device_id={axis: lax.rem(mine + off, n)}, device_id_type=MESH
            )
            return carry

        lax.fori_loop(1, n, one, 0)

    greet("sp", me, sp_n)
    greet("tp", tp, tp_n)

    def remote(src, dst, ss, rs, where):
        return pltpu.make_async_remote_copy(
            src_ref=src,
            dst_ref=dst,
            send_sem=ss,
            recv_sem=rs,
            device_id=where,
            device_id_type=MESH,
        )

    def each(n, body):
        def one(off, carry):
            body(off)
            return carry

        lax.fori_loop(1, n, one, 0)

    def sp_copy(off, src, dst, ss, rs):
        return remote(src, dst, ss.at[off], rs.at[off], {"sp": lax.rem(me + off, sp_n)})

    a = act[me].astype(F32)
    activation = (a / (1.0 + jnp.exp(-a))).astype(BF16)
    for i in range(3):
        loads[i].wait()
        mod_part[2 * i : 2 * i + 2, :] = dot(activation, modw[i])[0:2, :]
    mod_part[6:8, :] = jnp.zeros((2, W), F32)
    pl.semaphore_wait(barrier, sp_n - 1 + tp_n - 1)

    def m1(off):
        return sp_copy(off, mod_part, mod_recv.at[me], m1s, m1r)

    each(sp_n, lambda off: m1(off).start())

    def y_peer(off):
        return {"tp": lax.rem(my_y + off, y_n) * 2 + core}

    def y_source(off):
        return lax.rem(my_y - off + y_n, y_n) * 2 + core

    def wy(off, c):
        return remote(
            ow_h.at[c],
            ow_all.at[tp * H + c],
            wys.at[off * H + c],
            wyr.at[off * H + c],
            y_peer(off),
        )

    def wp(off, c):
        block = y_source(off) * H + c
        return remote(
            ow_all.at[block],
            ow_all.at[block],
            wps.at[off * H + c],
            wpr.at[off * H + c],
            {"tp": other},
        )

    for c in range(H):
        each(y_n, lambda off: wy(off, c).start())

    def relay_weight(c):
        def one(off):
            wy(off, c).wait_recv()
            wp(off, c).start()

        each(y_n, one)

    rows = 64
    loads[3].wait()
    loads[4].wait()

    def stat(source, base):
        height = min(rows, source.shape[0])

        def one(i, carry):
            r = pl.multiple_of(i * height, height)
            x = source[pl.ds(r, height), :].astype(F32)
            mean = jnp.mean(x * x, axis=-1, keepdims=True)
            inv[pl.ds(pl.multiple_of(base + r, height), height), :] = jnp.broadcast_to(
                lax.rsqrt(mean + EPS), (height, HEAD_DIM)
            )
            return carry

        lax.fori_loop(0, source.shape[0] // height, one, 0)

    stat(lat, 0)
    stat(ctx, T)

    each(sp_n, lambda off: m1(off).wait_recv())
    mod_recv[me] = mod_part[...]
    mod_sum[...] = lax.fori_loop(
        0, sp_n, lambda s, total: total + mod_recv[s], jnp.zeros((8, W), F32)
    )

    def m2(off):
        return remote(
            mod_sum,
            mod_all.at[tp],
            m2s.at[off],
            m2r.at[off],
            {"tp": lax.rem(tp + off, tp_n)},
        )

    each(tp_n, lambda off: m2(off).start())
    mod_all[tp] = mod_sum[...]
    loads[9].wait()

    def wown(c):
        block = tp * H + c
        return remote(
            ow_all.at[block], ow_all.at[block], wps.at[c], wpr.at[c], {"tp": other}
        )

    for c in range(H):
        wown(c).start()

    token = lax.broadcasted_iota(jnp.int32, (T, HEAD_DIM), 0)
    lane = lax.broadcasted_iota(jnp.int32, (T, HEAD_DIM), 1)
    place = me * T + token
    spot = jnp.where(lane < 64, place >> 6, place & 63).astype(F32)
    angle = spot * jnp.exp((lane & 31).astype(F32) * (-math.log(THETA) / 32.0))
    cosb[...] = jnp.cos(angle)
    sine = jnp.sin(angle)
    sinb[...] = jnp.where((lane & 32) == 0, -sine, sine)

    mt = 128

    def mix_rows(i, carry):
        r = pl.multiple_of(i * mt, mt)
        gap = (
            i * mt
            + lax.broadcasted_iota(jnp.int32, (mt, T), 0)
            - lax.broadcasted_iota(jnp.int32, (mt, T), 1)
        )
        gapf = gap.astype(F32)
        for h in range(H):
            weight = jnp.exp(jnp.where(gap >= 0, -fd[h] * gapf, bd[h] * gapf))
            mix[h, pl.ds(r, mt), :] = jnp.where(gap == 0, 2.0, weight).astype(BF16)
        return carry

    lax.fori_loop(0, T // mt, mix_rows, 0)

    each(tp_n, lambda off: m2(off).wait_recv())

    def modulate(source, base, row):
        height = min(rows, source.shape[0])
        tiles = source.shape[0] // height

        def one(i, carry):
            b = i // tiles
            r = pl.multiple_of(lax.rem(i, tiles) * height, height)
            cols = pl.ds(pl.multiple_of(b * W, W), W)
            out_rows = pl.ds(pl.multiple_of(base + r, height), height)
            x = source[pl.ds(r, height), cols].astype(F32) * inv[out_rows, 0:1]
            x = x * gain[:, cols]
            x = x * (1.0 + mod_all[b, 2 + row : 3 + row, :]) + mod_all[b, row : row + 1, :]
            hid[out_rows, cols] = x.astype(BF16)
            return carry

        lax.fori_loop(0, tp_n * tiles, one, 0)

    modulate(lat, 0, 0)
    modulate(ctx, T, 1)

    nt = min(256, W)

    def project(index, height):
        def one(j, carry):
            cols = pl.ds(pl.multiple_of(j * nt, nt), nt)
            proj[index, 0:height, cols] = dot(hid[0:height, :], wbuf[index, :, cols]).astype(BF16)
            return carry

        lax.fori_loop(0, W // nt, one, 0)

    loads[5].wait()
    project(1, T + CR)
    loads[6].wait()
    project(2, T + CR)

    scale = HEAD_DIM**-0.5
    step = token.astype(F32)
    low = (lane & 32) == 0
    cpos = (me * CR + lax.broadcasted_iota(jnp.int32, (CR, HEAD_DIM), 0)).astype(F32)
    ctotal = float(CR * sp_n)

    def put(ref, d, h, value):
        start = (d * H + h) * per
        ref[start : start + per] = value.reshape(per, R, HEAD_DIM).astype(BF16)

    for h in range(H):
        cols = slice(h * HEAD_DIM, (h + 1) * HEAD_DIM)
        ck = proj[1, T : T + CR, cols].astype(F32) * (scale * CONTEXT_LIFT)
        cv = proj[2, T : T + CR, cols]
        put(sc_send, 0, h, dot_rows((ck * jnp.exp(-fd[h] * (ctotal - 1.0 - cpos))).astype(BF16), cv))
        put(sc_send, 1, h, dot_rows((ck * jnp.exp(-bd[h] * cpos)).astype(BF16), cv))

    def scopy(off):
        return sp_copy(off, sc_send.at[lax.rem(me + off, sp_n)], sc_recv.at[me], scs, scr)

    def slcopy(off):
        return sp_copy(off, sl_send.at[lax.rem(me + off, sp_n)], sl_recv.at[me], sls, slr)

    def incopy(off):
        return sp_copy(off, in_send.at[lax.rem(me + off, sp_n)], in_recv.at[me], ins, inr)

    each(sp_n, lambda off: scopy(off).start())

    for h in range(H):
        cols = slice(h * HEAD_DIM, (h + 1) * HEAD_DIM)
        k = rotated(proj[1, 0:T, cols].astype(F32), cosb[...], sinb[...], low) * scale
        v = proj[2, 0:T, cols]
        put(sl_send, 0, h, dot_rows((k * jnp.exp(-fd[h] * (T - 1.0 - step))).astype(BF16), v))
        put(sl_send, 1, h, dot_rows((k * jnp.exp(-bd[h] * step)).astype(BF16), v))
        proj[1, 0:T, cols] = k.astype(BF16)

    each(sp_n, lambda off: slcopy(off).start())
    sc_recv[me] = sc_send[me]
    sl_recv[me] = sl_send[me]

    loads[7].wait()
    project(0, T)
    loads[8].wait()
    project(3, T)

    each(sp_n, lambda off: scopy(off).wait_recv())
    each(sp_n, lambda off: slcopy(off).wait_recv())
    backward = (me * R) // (H * HEAD_DIM)
    head = lax.rem((me * R) // HEAD_DIM, H)
    rate = jnp.where(backward == 1, bd[head], fd[head])
    span = jnp.exp(jnp.full((R, HEAD_DIM), -float(T), F32) * rate)
    start = lax.fori_loop(
        0, sp_n, lambda s, total: total + sc_recv[s].astype(F32), jnp.zeros((R, HEAD_DIM), F32)
    )

    def scan(lap, state):
        i = jnp.where(backward == 1, sp_n - 1 - lap, lap)
        in_send[i] = state.astype(BF16)
        return span * state + sl_recv[i].astype(F32)

    lax.fori_loop(0, sp_n, scan, start)
    each(sp_n, lambda off: incopy(off).start())
    in_recv[me] = in_send[me]

    for h in range(H):
        cols = slice(h * HEAD_DIM, (h + 1) * HEAD_DIM)
        q = rotated(proj[0, 0:T, cols].astype(F32), cosb[...], sinb[...], low).astype(BF16)
        proj[0, 0:T, cols] = q

        def score_rows(i, carry):
            r = pl.ds(pl.multiple_of(i * mt, mt), mt)
            s = dot_columns(proj[0, r, cols], proj[1, 0:T, cols]) * mix[h, r, :].astype(F32)
            local[r, cols] = dot(s.astype(BF16), proj[2, 0:T, cols])
            return carry

        lax.fori_loop(0, T // mt, score_rows, 0)

    each(sp_n, lambda off: incopy(off).wait_recv())

    def hview(block, h):
        return heads_all.at[block, :, pl.ds(h * HEAD_DIM, HEAD_DIM)]

    def hy(off, h):
        return remote(
            hview(tp, h), hview(tp, h), hys.at[off * H + h], hyr.at[off * H + h], y_peer(off)
        )

    def hp(off, h):
        block = y_source(off)
        return remote(
            hview(block, h),
            hview(block, h),
            hps.at[off * H + h],
            hpr.at[off * H + h],
            {"tp": other},
        )

    def hown(h):
        return remote(hview(tp, h), hview(tp, h), hps.at[h], hpr.at[h], {"tp": other})

    for h in range(H):
        cols = slice(h * HEAD_DIM, (h + 1) * HEAD_DIM)
        q = proj[0, 0:T, cols].astype(F32)
        at = h * per
        forward = in_recv[at : at + per].astype(F32).reshape(HEAD_DIM, HEAD_DIM).astype(BF16)
        at = (H + h) * per
        back = in_recv[at : at + per].astype(F32).reshape(HEAD_DIM, HEAD_DIM).astype(BF16)
        kept = (
            local[:, cols]
            + dot((q * jnp.exp(-fd[h] * (step + 1.0))).astype(BF16), forward)
            + dot((q * jnp.exp(-bd[h] * (T - step))).astype(BF16), back)
        )
        kept = kept * lax.rsqrt(jnp.mean(kept * kept, axis=-1, keepdims=True) + EPS)
        g = proj[3, 0:T, cols].astype(F32)
        heads_all[tp, :, cols] = (g / (1.0 + jnp.exp(-g)) * kept).astype(BF16)
        each(y_n, lambda off: hy(off, h).start())
        hown(h).start()

    for c in range(H):
        relay_weight(c)

    ot = 256

    def block_product(block, first, last):
        def one(j, carry):
            cols = pl.ds(pl.multiple_of(j * ot, ot), ot)
            value = None
            for c in range(0, H, 2 if H % 2 == 0 else 1):
                width = 2 if H % 2 == 0 else 1
                piece = heads_all[block, :, c * HEAD_DIM : (c + width) * HEAD_DIM]
                weight = ow_all[pl.ds(block * H + c, width), :, cols].reshape(
                    width * HEAD_DIM, ot
                )
                term = dot(piece, weight)
                value = term if value is None else value + term
            if not first:
                value = value + acc[:, cols]
            acc[:, cols] = value
            return carry

        lax.fori_loop(0, D // ot, one, 0)

    block_product(tp, True, False)
    for h in range(H):
        hown(h).wait_recv()
        wown(h).wait_recv()
    block_product(other, False, False)

    def far(off):
        for h in range(H):
            hy(off, h).wait_recv()
            hp(off, h).start()
        block_product(y_source(off), False, False)

    each(y_n, far)

    def farther(off):
        for h in range(H):
            hp(off, h).wait_recv()
            wp(off, h).wait_recv()
        block_product(lax.rem(my_y - off + y_n, y_n) * 2 + 1 - core, False, False)

    each(y_n, farther)

    def finish(i, carry):
        b = i // (T // rows)
        r = pl.multiple_of(lax.rem(i, T // rows) * rows, rows)
        cols = pl.ds(pl.multiple_of(b * W, W), W)
        value = lat[pl.ds(r, rows), cols].astype(F32) + mod_all[b, 4:5, :] * acc[pl.ds(r, rows), cols]
        out_v[pl.ds(r, rows), cols] = value.astype(BF16)
        return carry

    lax.fori_loop(0, tp_n * (T // rows), finish, 0)
    result = pltpu.make_async_copy(out_v, out_h, out_sem)
    result.start()

    each(sp_n, lambda off: m1(off).wait_send())
    each(tp_n, lambda off: m2(off).wait_send())
    each(sp_n, lambda off: scopy(off).wait_send())
    each(sp_n, lambda off: slcopy(off).wait_send())
    each(sp_n, lambda off: incopy(off).wait_send())
    for h in range(H):
        wown(h).wait_send()
        hown(h).wait_send()

    def settle(off):
        for h in range(H):
            wy(off, h).wait_send()
            wp(off, h).wait_send()
            hy(off, h).wait_send()
            hp(off, h).wait_send()

    each(y_n, settle)
    result.wait()


def local_program(
    sp_n,
    tp_n,
    latent,
    context,
    condition,
    context_condition,
    shift_weight,
    scale_weight,
    mod_gate_weight,
    norm_gain,
    query_weight,
    key_weight,
    value_weight,
    gate_weight,
    forward_decay,
    backward_decay,
    out_weight,
):
    T, D = latent.shape
    CR = context.shape[0]
    MR, W = shift_weight.shape
    H = W // HEAD_DIM
    R = 2 * H * HEAD_DIM // sp_n
    pair = jnp.stack([condition, context_condition]).reshape(2, sp_n, MR)
    act = jnp.pad(jnp.transpose(pair, (1, 0, 2)), ((0, 0), (0, 14), (0, 0)))
    gain = norm_gain.astype(F32).reshape(1, D)
    ow = out_weight.reshape(H, HEAD_DIM, D)
    y_n = tp_n // 2
    vm = pl.BlockSpec(memory_space=pltpu.VMEM)
    sm = pl.BlockSpec(memory_space=pltpu.SMEM)
    hb = pl.BlockSpec(memory_space=pl.ANY)
    V = pltpu.VMEM
    dma = pltpu.SemaphoreType.DMA
    state = V((sp_n, R, HEAD_DIM), BF16)
    return pl.pallas_call(
        functools.partial(kernel, sp_n, tp_n),
        out_shape=jax.ShapeDtypeStruct((T, D), BF16),
        in_specs=[vm, vm, sm, sm] + [hb] * 10,
        out_specs=hb,
        scratch_shapes=[
            V((T, D), BF16),
            V((CR, D), BF16),
            V((3, MR, W), BF16),
            V((4, D, W), BF16),
            V((T + CR, D), BF16),
            V((8, W), F32),
            V((sp_n, 8, W), F32),
            V((8, W), F32),
            V((tp_n, 8, W), F32),
            V((T + CR, HEAD_DIM), F32),
            V((T, HEAD_DIM), F32),
            V((T, HEAD_DIM), F32),
            V((4, T + CR, W), BF16),
            V((H, T, T), BF16),
            V((T, W), F32),
            V((tp_n, T, W), BF16),
            V((tp_n * H, HEAD_DIM, D), BF16),
            V((T, D), F32),
            V((T, D), BF16),
            state,
            state,
            state,
            state,
            state,
            state,
            dma((10,)),
            dma((sp_n,)),
            dma((sp_n,)),
            dma((tp_n,)),
            dma((tp_n,)),
        ]
        + [dma((sp_n,))] * 6
        + [dma((y_n * H,))] * 8
        + [dma],
        compiler_params=pltpu.CompilerParams(
            collective_id=0, has_side_effects=True, vmem_limit_bytes=60 * 1024 * 1024
        ),
    )(
        act,
        gain,
        forward_decay,
        backward_decay,
        latent,
        context,
        shift_weight,
        scale_weight,
        mod_gate_weight,
        query_weight,
        key_weight,
        value_weight,
        gate_weight,
        ow,
    )


def solution(mesh):
    placed = (
        P("sp", None),
        P("sp", None),
        P(),
        P(),
        P("sp", "tp"),
        P("sp", "tp"),
        P("sp", "tp"),
        P(),
        P(None, "tp"),
        P(None, "tp"),
        P(None, "tp"),
        P(None, "tp"),
        P("tp"),
        P("tp"),
        P("tp", None),
    )
    return jax.shard_map(
        functools.partial(local_program, mesh.shape["sp"], mesh.shape["tp"]),
        mesh=mesh,
        in_specs=placed,
        out_specs=P("sp", None),
        check_vma=False,
    )
```

```python
import functools
import math

import jax
import jax.numpy as jnp
from jax import lax
from jax.experimental import pallas as pl
from jax.experimental.pallas import tpu as pltpu
from jax.sharding import PartitionSpec as P

HEAD_DIM = 128
GRID_W = 64
EPS = 1e-06
THETA = 10000.0
CONTEXT_LIFT = 3.0
MESH = pl.DeviceIdType.MESH
F32 = jnp.float32
BF16 = jnp.bfloat16


def dot(a, b):
    return jnp.dot(a, b, preferred_element_type=F32)


def dot_rows(a, b):
    return lax.dot_general(a, b, (((0,), (0,)), ((), ())), preferred_element_type=F32)


def dot_columns(a, b):
    return lax.dot_general(a, b, (((1,), (1,)), ((), ())), preferred_element_type=F32)


def rotated(x, cosines, sines, low):
    partner = jnp.where(low, pltpu.roll(x, HEAD_DIM - 32, 1), pltpu.roll(x, 32, 1))
    return x * cosines + partner * sines


def kernel(sp_n, tp_n, small_n, *refs):
    act = refs[1] if small_n == 2 else None
    body(sp_n, tp_n, act, refs[0], *refs[small_n:])


def body(
    sp_n,
    tp_n,
    act,
    gain,
    fd,
    bd,
    latent_h,
    context_h,
    shift_h,
    scale_h,
    gate_h,
    wq_h,
    wk_h,
    wv_h,
    wg_h,
    ow_h,
    out_h,
    lat,
    ctx,
    modw,
    wbuf,
    hid,
    mod_part,
    mod_recv,
    mod_sum,
    mod_all,
    inv,
    cosb,
    sinb,
    proj,
    mix,
    local,
    heads_all,
    ow_all,
    acc,
    gates,
    out_v,
    sc_send,
    sc_recv,
    sl_send,
    sl_recv,
    in_send,
    in_recv,
    load_sem,
    m1s,
    m1r,
    m2s,
    m2r,
    scs,
    scr,
    sls,
    slr,
    ins,
    inr,
    wos,
    wor,
    wys,
    wyr,
    wxs,
    wxr,
    wps,
    wpr,
    wqs,
    wqr,
    hys,
    hyr,
    hps,
    hpr,
    out_sem,
):
    me = lax.axis_index("sp")
    tp = lax.axis_index("tp")
    y_n = tp_n // 2
    my_y = tp // 2
    core = lax.rem(tp, 2)
    other = my_y * 2 + 1 - core
    T, D = lat.shape
    CR = ctx.shape[0]
    W = wbuf.shape[2]
    H = W // HEAD_DIM
    R = sl_send.shape[1]
    per = HEAD_DIM // R
    CN = ow_h.shape[0]
    half = CN // 2
    parity = lax.rem(me, 2)
    beside = me + 1 - 2 * parity

    loads = [
        pltpu.make_async_copy(src, dst, load_sem.at[i])
        for i, (src, dst) in enumerate(
            [
                (shift_h, modw.at[0]),
                (scale_h, modw.at[1]),
                (gate_h, modw.at[2]),
                (latent_h, lat),
                (context_h, ctx),
                (wk_h, wbuf.at[1]),
                (wv_h, wbuf.at[2]),
                (wq_h, wbuf.at[0]),
                (wg_h, wbuf.at[3]),
                (ow_h, ow_all.at[pl.ds(tp * CN, CN)]),
            ]
        )
    ]
    for load in loads:
        load.start()

    barrier = pltpu.get_barrier_semaphore()

    def greet(axis, mine, n):
        def one(off, carry):
            pl.semaphore_signal(
                barrier, inc=1, device_id={axis: lax.rem(mine + off, n)}, device_id_type=MESH
            )
            return carry

        lax.fori_loop(1, n, one, 0)

    greet("sp", me, sp_n)
    greet("tp", tp, tp_n)

    def remote(src, dst, ss, rs, where):
        return pltpu.make_async_remote_copy(
            src_ref=src,
            dst_ref=dst,
            send_sem=ss,
            recv_sem=rs,
            device_id=where,
            device_id_type=MESH,
        )

    def each(n, body):
        def one(off, carry):
            body(off)
            return carry

        lax.fori_loop(1, n, one, 0)

    def sp_copy(off, src, dst, ss, rs):
        return remote(src, dst, ss.at[off], rs.at[off], {"sp": lax.rem(me + off, sp_n)})

    MR = modw.shape[1]
    if act is None:
        a = gain[0:2, pl.ds(pl.multiple_of(me * MR, MR), MR)]
        a = jnp.concatenate([a, jnp.zeros((6, MR), F32)], axis=0)
    else:
        a = act[me].astype(F32)
    activation = (a / (1.0 + jnp.exp(-a))).astype(BF16)
    for i in range(3):
        loads[i].wait()
        mod_part[2 * i : 2 * i + 2, :] = dot(activation, modw[i])[0:2, :]
    mod_part[6:8, :] = jnp.zeros((2, W), F32)
    pl.semaphore_wait(barrier, sp_n - 1 + tp_n - 1)

    def m1(off):
        return sp_copy(off, mod_part, mod_recv.at[me], m1s, m1r)

    each(sp_n, lambda off: m1(off).start())

    def y_peer(off):
        return {"tp": lax.rem(my_y + off, y_n) * 2 + core}

    def y_source(off):
        return lax.rem(my_y - off + y_n, y_n) * 2 + core

    rows = 64
    loads[3].wait()
    loads[4].wait()

    def stat(source, base):
        height = min(rows, source.shape[0])

        def one(i, carry):
            r = pl.multiple_of(i * height, height)
            x = source[pl.ds(r, height), :].astype(F32)
            mean = jnp.mean(x * x, axis=-1, keepdims=True)
            inv[pl.ds(pl.multiple_of(base + r, height), height), :] = jnp.broadcast_to(
                lax.rsqrt(mean + EPS), (height, HEAD_DIM)
            )
            return carry

        lax.fori_loop(0, source.shape[0] // height, one, 0)

    stat(lat, 0)
    stat(ctx, T)

    each(sp_n, lambda off: m1(off).wait_recv())
    mod_recv[me] = mod_part[...]
    mod_sum[...] = lax.fori_loop(
        0, sp_n, lambda s, total: total + mod_recv[s], jnp.zeros((8, W), F32)
    )

    def m2(off):
        return remote(
            mod_sum,
            mod_all.at[tp],
            m2s.at[off],
            m2r.at[off],
            {"tp": lax.rem(tp + off, tp_n)},
        )

    each(tp_n, lambda off: m2(off).start())
    mod_all[tp] = mod_sum[...]

    token = lax.broadcasted_iota(jnp.int32, (T, HEAD_DIM), 0)
    lane = lax.broadcasted_iota(jnp.int32, (T, HEAD_DIM), 1)
    place = me * T + token
    spot = jnp.where(lane < 64, place >> 6, place & 63).astype(F32)
    angle = spot * jnp.exp((lane & 31).astype(F32) * (-math.log(THETA) / 32.0))
    cosb[...] = jnp.cos(angle)
    sine = jnp.sin(angle)
    sinb[...] = jnp.where((lane & 32) == 0, -sine, sine)

    mt = 128

    def mix_rows(i, carry):
        r = pl.multiple_of(i * mt, mt)
        gap = (
            i * mt
            + lax.broadcasted_iota(jnp.int32, (mt, T), 0)
            - lax.broadcasted_iota(jnp.int32, (mt, T), 1)
        )
        gapf = gap.astype(F32)
        for h in range(H):
            weight = jnp.exp(jnp.where(gap >= 0, -fd[h] * gapf, bd[h] * gapf))
            mix[h, pl.ds(r, mt), :] = jnp.where(gap == 0, 2.0, weight).astype(BF16)
        return carry

    lax.fori_loop(0, T // mt, mix_rows, 0)

    each(tp_n, lambda off: m2(off).wait_recv())

    def gate_row(b, carry):
        gates[0:1, pl.ds(pl.multiple_of(b * W, W), W)] = mod_all[b, 4:5, :]
        return carry

    lax.fori_loop(0, tp_n, gate_row, 0)

    wown = remote(ow_h, ow_all.at[pl.ds(tp * CN, CN)], wos.at[0], wor.at[0], {"tp": other})

    def wy(off, i):
        c = parity * half + i
        return remote(
            ow_h.at[c],
            ow_all.at[tp * CN + c],
            wys.at[off * half + i],
            wyr.at[off * half + i],
            y_peer(off),
        )

    def passed(off, i, side, ss, rs, where):
        c = ow_all.at[y_source(off) * CN + side * half + i]
        return remote(c, c, ss.at[off * half + i], rs.at[off * half + i], where)

    def wx(off, i):
        return passed(off, i, parity, wxs, wxr, {"sp": beside})

    def wp(off, i):
        return passed(off, i, parity, wps, wpr, {"tp": other})

    def wq(off, i):
        return passed(off, i, 1 - parity, wqs, wqr, {"tp": other})

    for i in range(half):
        each(y_n, lambda off: wy(off, i).start())
    wown.start()

    def relay_y(i):
        def one(off):
            wy(off, i).wait_recv()
            wx(off, i).start()
            wp(off, i).start()

        each(y_n, one)

    def relay_x(i):
        def one(off):
            wx(off, i).wait_recv()
            wq(off, i).start()

        each(y_n, one)

    quarter = max(half // 4, 1)

    def relay(which, phase):
        for i in range(phase * quarter, min((phase + 1) * quarter, half)):
            which(i)

    def modulate(source, base, row):
        height = min(rows, source.shape[0])
        tiles = source.shape[0] // height

        def one(i, carry):
            b = i // tiles
            r = pl.multiple_of(lax.rem(i, tiles) * height, height)
            cols = pl.ds(pl.multiple_of(b * W, W), W)
            out_rows = pl.ds(pl.multiple_of(base + r, height), height)
            level = inv[out_rows, :]
            lift = gain[gain.shape[0] - 1 :, cols] * (1.0 + mod_all[b, 2 + row : 3 + row, :])
            shift = mod_all[b, row : row + 1, :]
            x = source[pl.ds(r, height), cols].astype(F32)
            for h in range(H):
                c = slice(h * HEAD_DIM, (h + 1) * HEAD_DIM)
                to = pl.ds(pl.multiple_of(b * W + h * HEAD_DIM, HEAD_DIM), HEAD_DIM)
                hid[out_rows, to] = (x[:, c] * level * lift[:, c] + shift[:, c]).astype(BF16)
            return carry

        lax.fori_loop(0, tp_n * tiles, one, 0)

    modulate(lat, 0, 0)
    modulate(ctx, T, 1)

    nt = min(256, W)

    def project(index, height):
        def one(j, carry):
            cols = pl.ds(pl.multiple_of(j * nt, nt), nt)
            proj[index, 0:height, cols] = dot(hid[0:height, :], wbuf[index, :, cols]).astype(BF16)
            return carry

        lax.fori_loop(0, W // nt, one, 0)

    loads[5].wait()
    project(1, T + CR)
    loads[6].wait()
    project(2, T + CR)

    scale = HEAD_DIM**-0.5
    step = token.astype(F32)
    low = (lane & 32) == 0
    cpos = (me * CR + lax.broadcasted_iota(jnp.int32, (CR, HEAD_DIM), 0)).astype(F32)
    ctotal = float(CR * sp_n)

    def put(ref, d, h, value):
        start = (d * H + h) * per
        ref[start : start + per] = value.reshape(per, R, HEAD_DIM).astype(BF16)

    for h in range(H):
        cols = slice(h * HEAD_DIM, (h + 1) * HEAD_DIM)
        ck = proj[1, T : T + CR, cols].astype(F32) * (scale * CONTEXT_LIFT)
        cv = proj[2, T : T + CR, cols]
        put(sc_send, 0, h, dot_rows((ck * jnp.exp(-fd[h] * (ctotal - 1.0 - cpos))).astype(BF16), cv))
        put(sc_send, 1, h, dot_rows((ck * jnp.exp(-bd[h] * cpos)).astype(BF16), cv))

    def scopy(off):
        return sp_copy(off, sc_send.at[lax.rem(me + off, sp_n)], sc_recv.at[me], scs, scr)

    def slcopy(off):
        return sp_copy(off, sl_send.at[lax.rem(me + off, sp_n)], sl_recv.at[me], sls, slr)

    def incopy(off):
        return sp_copy(off, in_send.at[lax.rem(me + off, sp_n)], in_recv.at[me], ins, inr)

    each(sp_n, lambda off: scopy(off).start())

    for h in range(H):
        cols = slice(h * HEAD_DIM, (h + 1) * HEAD_DIM)
        k = rotated(proj[1, 0:T, cols].astype(F32), cosb[...], sinb[...], low) * scale
        v = proj[2, 0:T, cols]
        put(sl_send, 0, h, dot_rows((k * jnp.exp(-fd[h] * (T - 1.0 - step))).astype(BF16), v))
        put(sl_send, 1, h, dot_rows((k * jnp.exp(-bd[h] * step)).astype(BF16), v))
        proj[1, 0:T, cols] = k.astype(BF16)

    each(sp_n, lambda off: slcopy(off).start())
    relay(relay_y, 0)
    sc_recv[me] = sc_send[me]
    sl_recv[me] = sl_send[me]

    loads[7].wait()
    project(0, T)
    loads[8].wait()
    project(3, T)

    relay(relay_y, 1)
    each(sp_n, lambda off: scopy(off).wait_recv())
    each(sp_n, lambda off: slcopy(off).wait_recv())
    backward = (me * R) // (H * HEAD_DIM)
    head = lax.rem((me * R) // HEAD_DIM, H)
    rate = jnp.where(backward == 1, bd[head], fd[head])
    span = jnp.exp(jnp.full((R, HEAD_DIM), -float(T), F32) * rate)
    start = lax.fori_loop(
        0, sp_n, lambda s, total: total + sc_recv[s].astype(F32), jnp.zeros((R, HEAD_DIM), F32)
    )

    def scan(lap, state):
        i = jnp.where(backward == 1, sp_n - 1 - lap, lap)
        in_send[i] = state.astype(BF16)
        return span * state + sl_recv[i].astype(F32)

    lax.fori_loop(0, sp_n, scan, start)
    each(sp_n, lambda off: incopy(off).start())
    in_recv[me] = in_send[me]
    relay(relay_y, 2)

    st = 256 if T % 256 == 0 else mt
    for h in range(H):
        cols = slice(h * HEAD_DIM, (h + 1) * HEAD_DIM)
        q = rotated(proj[0, 0:T, cols].astype(F32), cosb[...], sinb[...], low).astype(BF16)
        proj[0, 0:T, cols] = q

        def score_rows(i, carry):
            r = pl.ds(pl.multiple_of(i * st, st), st)
            s = dot_columns(proj[0, r, cols], proj[1, 0:T, cols]) * mix[h, r, :].astype(F32)
            local[r, cols] = dot(s.astype(BF16), proj[2, 0:T, cols])
            return carry

        lax.fori_loop(0, T // st, score_rows, 0)

    relay(relay_y, 3)
    relay(relay_x, 0)
    each(sp_n, lambda off: incopy(off).wait_recv())

    def hview(block, h):
        return heads_all.at[block, :, pl.ds(h * HEAD_DIM, HEAD_DIM)]

    def hy(off, h):
        return remote(
            hview(tp, h), hview(tp, h), hys.at[off * H + h], hyr.at[off * H + h], y_peer(off)
        )

    def hp(off, h):
        block = y_source(off)
        return remote(
            hview(block, h),
            hview(block, h),
            hps.at[off * H + h],
            hpr.at[off * H + h],
            {"tp": other},
        )

    def hown(h):
        return remote(hview(tp, h), hview(tp, h), hps.at[h], hpr.at[h], {"tp": other})

    for h in range(H):
        cols = slice(h * HEAD_DIM, (h + 1) * HEAD_DIM)
        q = proj[0, 0:T, cols].astype(F32)
        at = h * per
        forward = in_recv[at : at + per].astype(F32).reshape(HEAD_DIM, HEAD_DIM).astype(BF16)
        at = (H + h) * per
        back = in_recv[at : at + per].astype(F32).reshape(HEAD_DIM, HEAD_DIM).astype(BF16)
        kept = (
            local[:, cols]
            + dot((q * jnp.exp(-fd[h] * (step + 1.0))).astype(BF16), forward)
            + dot((q * jnp.exp(-bd[h] * (T - step))).astype(BF16), back)
        )
        kept = kept * lax.rsqrt(jnp.mean(kept * kept, axis=-1, keepdims=True) + EPS)
        g = proj[3, 0:T, cols].astype(F32)
        heads_all[tp, :, cols] = (g / (1.0 + jnp.exp(-g)) * kept).astype(BF16)
        each(y_n, lambda off: hy(off, h).start())
        hown(h).start()

    relay(relay_x, 1)

    ot = min(256, W)

    def out_tile(j):
        cols = pl.ds(pl.multiple_of(j * ot, ot), ot)
        return pltpu.make_async_copy(out_v.at[:, cols], out_h.at[:, cols], out_sem.at[j])

    def block_product(block, first=False, last=False):
        def one(j, carry):
            cols = pl.ds(pl.multiple_of(j * ot, ot), ot)
            weight = ow_all[pl.ds(block * CN, CN), :, cols].reshape(W, ot)
            value = dot(heads_all[block], weight)
            if not first:
                value = value + acc[:, cols]
            if last:
                value = lat[:, cols].astype(F32) + gates[0:1, cols] * value
                out_v[:, cols] = value.astype(BF16)
                out_tile(j).start()
            else:
                acc[:, cols] = value
            return carry

        lax.fori_loop(0, D // ot, one, 0)

    loads[9].wait()
    block_product(tp, first=True)
    for h in range(H):
        hown(h).wait_recv()
    wown.wait_recv()
    relay(relay_x, 2)
    block_product(other)
    relay(relay_x, 3)

    def far(off):
        for h in range(H):
            hy(off, h).wait_recv()
            hp(off, h).start()
        block_product(y_source(off))

    each(y_n, far)

    def farther(off):
        for h in range(H):
            hp(off, h).wait_recv()
        for i in range(half):
            wp(off, i).wait_recv()
            wq(off, i).wait_recv()

    def farther_block(off):
        return y_source(off) + 1 - 2 * core

    def middle(off):
        farther(off)
        block_product(farther_block(off))

    each(y_n - 1, middle)
    farther(y_n - 1)
    block_product(farther_block(y_n - 1), last=True)

    each(sp_n, lambda off: m1(off).wait_send())
    each(tp_n, lambda off: m2(off).wait_send())
    each(sp_n, lambda off: scopy(off).wait_send())
    each(sp_n, lambda off: slcopy(off).wait_send())
    each(sp_n, lambda off: incopy(off).wait_send())
    wown.wait_send()
    for h in range(H):
        hown(h).wait_send()

    def settle(off):
        for i in range(half):
            wy(off, i).wait_send()
            wx(off, i).wait_send()
            wp(off, i).wait_send()
            wq(off, i).wait_send()
        for h in range(H):
            hy(off, h).wait_send()
            hp(off, h).wait_send()

    each(y_n, settle)

    def written(j, carry):
        out_tile(j).wait()
        return carry

    lax.fori_loop(0, D // ot, written, 0)


def local_program(
    sp_n,
    tp_n,
    latent,
    context,
    condition,
    context_condition,
    shift_weight,
    scale_weight,
    mod_gate_weight,
    norm_gain,
    query_weight,
    key_weight,
    value_weight,
    gate_weight,
    forward_decay,
    backward_decay,
    out_weight,
):
    T, D = latent.shape
    CR = context.shape[0]
    MR, W = shift_weight.shape
    H = W // HEAD_DIM
    R = 2 * H * HEAD_DIM // sp_n
    CN = W // 64
    ow = out_weight.reshape(CN, W // CN, D)
    if MR % HEAD_DIM == 0:
        rows = jnp.concatenate([condition, context_condition, norm_gain])
        small = [rows.astype(F32).reshape(3, D)]
    else:
        pair = jnp.stack([condition, context_condition]).reshape(2, sp_n, MR)
        act = jnp.pad(jnp.transpose(pair, (1, 0, 2)), ((0, 0), (0, 14), (0, 0)))
        small = [norm_gain.astype(F32).reshape(1, D), act]
    y_n = tp_n // 2
    vm = pl.BlockSpec(memory_space=pltpu.VMEM)
    sm = pl.BlockSpec(memory_space=pltpu.SMEM)
    hb = pl.BlockSpec(memory_space=pl.ANY)
    V = pltpu.VMEM
    dma = pltpu.SemaphoreType.DMA
    state = V((sp_n, R, HEAD_DIM), BF16)
    return pl.pallas_call(
        functools.partial(kernel, sp_n, tp_n, len(small)),
        out_shape=jax.ShapeDtypeStruct((T, D), BF16),
        in_specs=[vm] * len(small) + [sm, sm] + [hb] * 10,
        out_specs=hb,
        scratch_shapes=[
            V((T, D), BF16),
            V((CR, D), BF16),
            V((3, MR, W), BF16),
            V((4, D, W), BF16),
            V((T + CR, D), BF16),
            V((8, W), F32),
            V((sp_n, 8, W), F32),
            V((8, W), F32),
            V((tp_n, 8, W), F32),
            V((T + CR, HEAD_DIM), F32),
            V((T, HEAD_DIM), F32),
            V((T, HEAD_DIM), F32),
            V((4, T + CR, W), BF16),
            V((H, T, T), BF16),
            V((T, W), F32),
            V((tp_n, T, W), BF16),
            V((tp_n * CN, W // CN, D), BF16),
            V((T, D), F32),
            V((8, D), F32),
            V((T, D), BF16),
            state,
            state,
            state,
            state,
            state,
            state,
            dma((10,)),
            dma((sp_n,)),
            dma((sp_n,)),
            dma((tp_n,)),
            dma((tp_n,)),
        ]
        + [dma((sp_n,))] * 6
        + [dma((1,))] * 2
        + [dma((y_n * CN // 2,))] * 8
        + [dma((y_n * H,))] * 4
        + [dma((D // min(256, W),))],
        compiler_params=pltpu.CompilerParams(
            collective_id=0, has_side_effects=True, vmem_limit_bytes=60 * 1024 * 1024
        ),
    )(
        *small,
        forward_decay,
        backward_decay,
        latent,
        context,
        shift_weight,
        scale_weight,
        mod_gate_weight,
        query_weight,
        key_weight,
        value_weight,
        gate_weight,
        ow,
    )


def solution(mesh):
    placed = (
        P("sp", None),
        P("sp", None),
        P(),
        P(),
        P("sp", "tp"),
        P("sp", "tp"),
        P("sp", "tp"),
        P(),
        P(None, "tp"),
        P(None, "tp"),
        P(None, "tp"),
        P(None, "tp"),
        P("tp"),
        P("tp"),
        P("tp", None),
    )
    return jax.shard_map(
        functools.partial(local_program, mesh.shape["sp"], mesh.shape["tp"]),
        mesh=mesh,
        in_specs=placed,
        out_specs=P("sp", None),
        check_vma=False,
    )
```

```python
import functools
import math

import jax
import jax.numpy as jnp
from jax import lax
from jax.experimental import pallas as pl
from jax.experimental.pallas import tpu as pltpu
from jax.sharding import PartitionSpec as P

HEAD_DIM = 128
GRID_W = 64
EPS = 1e-06
THETA = 10000.0
CONTEXT_LIFT = 3.0
MESH = pl.DeviceIdType.MESH
F32 = jnp.float32
BF16 = jnp.bfloat16


def dot(a, b):
    return jnp.dot(a, b, preferred_element_type=F32)


def dot_rows(a, b):
    return lax.dot_general(a, b, (((0,), (0,)), ((), ())), preferred_element_type=F32)


def dot_columns(a, b):
    return lax.dot_general(a, b, (((1,), (1,)), ((), ())), preferred_element_type=F32)


def rotated(x, cosines, sines, low):
    partner = jnp.where(low, pltpu.roll(x, HEAD_DIM - 32, 1), pltpu.roll(x, 32, 1))
    return x * cosines + partner * sines


def kernel(sp_n, tp_n, small_n, *refs):
    act = refs[1] if small_n == 2 else None
    body(sp_n, tp_n, act, refs[0], *refs[small_n:])


def body(
    sp_n,
    tp_n,
    act,
    gain,
    fd,
    bd,
    latent_h,
    context_h,
    shift_h,
    scale_h,
    gate_h,
    wq_h,
    wk_h,
    wv_h,
    wg_h,
    ow_h,
    out_h,
    lat,
    ctx,
    modw,
    wbuf,
    hid,
    mod_part,
    mod_recv,
    mod_sum,
    mod_all,
    inv,
    cosb,
    sinb,
    proj,
    mix,
    local,
    heads_all,
    ow_all,
    acc,
    gates,
    out_v,
    sc_send,
    sc_recv,
    sl_send,
    sl_recv,
    in_send,
    in_recv,
    load_sem,
    m1s,
    m1r,
    m2s,
    m2r,
    scs,
    scr,
    sls,
    slr,
    ins,
    inr,
    wos,
    wor,
    wys,
    wyr,
    wxs,
    wxr,
    wps,
    wpr,
    wqs,
    wqr,
    hys,
    hyr,
    hps,
    hpr,
    out_sem,
):
    me = lax.axis_index("sp")
    tp = lax.axis_index("tp")
    y_n = tp_n // 2
    my_y = tp // 2
    core = lax.rem(tp, 2)
    other = my_y * 2 + 1 - core
    T, D = lat.shape
    CR = ctx.shape[0]
    W = wbuf.shape[2]
    H = W // HEAD_DIM
    R = sl_send.shape[1]
    per = HEAD_DIM // R
    CN = ow_h.shape[0]
    half = CN // 2
    parity = lax.rem(me, 2)
    beside = me + 1 - 2 * parity

    loads = [
        pltpu.make_async_copy(src, dst, load_sem.at[i])
        for i, (src, dst) in enumerate(
            [
                (shift_h, modw.at[0]),
                (scale_h, modw.at[1]),
                (gate_h, modw.at[2]),
                (latent_h, lat),
                (context_h, ctx),
                (wk_h, wbuf.at[1]),
                (wv_h, wbuf.at[2]),
                (wq_h, wbuf.at[0]),
                (wg_h, wbuf.at[3]),
                (ow_h, ow_all.at[pl.ds(tp * CN, CN)]),
            ]
        )
    ]
    for load in loads:
        load.start()

    barrier = pltpu.get_barrier_semaphore()

    def greet(axis, mine, n):
        def one(off, carry):
            pl.semaphore_signal(
                barrier, inc=1, device_id={axis: lax.rem(mine + off, n)}, device_id_type=MESH
            )
            return carry

        lax.fori_loop(1, n, one, 0)

    greet("sp", me, sp_n)
    greet("tp", tp, tp_n)

    def remote(src, dst, ss, rs, where):
        return pltpu.make_async_remote_copy(
            src_ref=src,
            dst_ref=dst,
            send_sem=ss,
            recv_sem=rs,
            device_id=where,
            device_id_type=MESH,
        )

    def each(n, body):
        def one(off, carry):
            body(off)
            return carry

        lax.fori_loop(1, n, one, 0)

    def sp_copy(off, src, dst, ss, rs):
        return remote(src, dst, ss.at[off], rs.at[off], {"sp": lax.rem(me + off, sp_n)})

    MR = modw.shape[1]
    if act is None:
        a = gain[0:2, pl.ds(pl.multiple_of(me * MR, MR), MR)]
        a = jnp.concatenate([a, jnp.zeros((6, MR), F32)], axis=0)
    else:
        a = act[me].astype(F32)
    activation = (a / (1.0 + jnp.exp(-a))).astype(BF16)
    for i in range(3):
        loads[i].wait()
        mod_part[2 * i : 2 * i + 2, :] = dot(activation, modw[i])[0:2, :]
    mod_part[6:8, :] = jnp.zeros((2, W), F32)
    pl.semaphore_wait(barrier, sp_n - 1 + tp_n - 1)

    def m1(off):
        return sp_copy(off, mod_part, mod_recv.at[me], m1s, m1r)

    each(sp_n, lambda off: m1(off).start())

    def y_peer(off):
        return {"tp": lax.rem(my_y + off, y_n) * 2 + core}

    def y_source(off):
        return lax.rem(my_y - off + y_n, y_n) * 2 + core

    rows = 64
    loads[3].wait()
    loads[4].wait()

    def stat(source, base):
        height = min(rows, source.shape[0])

        def one(i, carry):
            r = pl.multiple_of(i * height, height)
            x = source[pl.ds(r, height), :].astype(F32)
            mean = jnp.mean(x * x, axis=-1, keepdims=True)
            inv[pl.ds(pl.multiple_of(base + r, height), height), :] = jnp.broadcast_to(
                lax.rsqrt(mean + EPS), (height, HEAD_DIM)
            )
            return carry

        lax.fori_loop(0, source.shape[0] // height, one, 0)

    stat(lat, 0)
    stat(ctx, T)

    each(sp_n, lambda off: m1(off).wait_recv())
    mod_recv[me] = mod_part[...]
    mod_sum[...] = lax.fori_loop(
        0, sp_n, lambda s, total: total + mod_recv[s], jnp.zeros((8, W), F32)
    )

    def m2(off):
        return remote(
            mod_sum,
            mod_all.at[tp],
            m2s.at[off],
            m2r.at[off],
            {"tp": lax.rem(tp + off, tp_n)},
        )

    each(tp_n, lambda off: m2(off).start())
    mod_all[tp] = mod_sum[...]

    token = lax.broadcasted_iota(jnp.int32, (T, HEAD_DIM), 0)
    lane = lax.broadcasted_iota(jnp.int32, (T, HEAD_DIM), 1)
    place = me * T + token
    spot = jnp.where(lane < 64, place >> 6, place & 63).astype(F32)
    angle = spot * jnp.exp((lane & 31).astype(F32) * (-math.log(THETA) / 32.0))
    cosb[...] = jnp.cos(angle)
    sine = jnp.sin(angle)
    sinb[...] = jnp.where((lane & 32) == 0, -sine, sine)

    mt = 128

    def mix_rows(i, carry):
        r = pl.multiple_of(i * mt, mt)
        gap = (
            i * mt
            + lax.broadcasted_iota(jnp.int32, (mt, T), 0)
            - lax.broadcasted_iota(jnp.int32, (mt, T), 1)
        )
        gapf = gap.astype(F32)
        for h in range(H):
            weight = jnp.exp(jnp.where(gap >= 0, -fd[h] * gapf, bd[h] * gapf))
            mix[h, pl.ds(r, mt), :] = jnp.where(gap == 0, 2.0, weight).astype(BF16)
        return carry

    lax.fori_loop(0, T // mt, mix_rows, 0)

    each(tp_n, lambda off: m2(off).wait_recv())

    def gate_row(b, carry):
        gates[0:1, pl.ds(pl.multiple_of(b * W, W), W)] = mod_all[b, 4:5, :]
        return carry

    lax.fori_loop(0, tp_n, gate_row, 0)

    wown = remote(ow_h, ow_all.at[pl.ds(tp * CN, CN)], wos.at[0], wor.at[0], {"tp": other})

    def wy(off, i):
        c = parity * half + i
        return remote(
            ow_h.at[c],
            ow_all.at[tp * CN + c],
            wys.at[off * half + i],
            wyr.at[off * half + i],
            y_peer(off),
        )

    def passed(off, i, side, ss, rs, where):
        c = ow_all.at[y_source(off) * CN + side * half + i]
        return remote(c, c, ss.at[off * half + i], rs.at[off * half + i], where)

    def wx(off, i):
        return passed(off, i, parity, wxs, wxr, {"sp": beside})

    def wp(off, i):
        return passed(off, i, parity, wps, wpr, {"tp": other})

    def wq(off, i):
        return passed(off, i, 1 - parity, wqs, wqr, {"tp": other})

    for i in range(half):
        each(y_n, lambda off: wy(off, i).start())
    wown.start()

    def relay_y(i):
        def one(off):
            wy(off, i).wait_recv()
            wx(off, i).start()
            wp(off, i).start()

        each(y_n, one)

    def relay_x(i):
        def one(off):
            wx(off, i).wait_recv()
            wq(off, i).start()

        each(y_n, one)

    quarter = max(half // 4, 1)

    def relay(which, phase):
        for i in range(phase * quarter, min((phase + 1) * quarter, half)):
            which(i)

    def modulate(source, base, row):
        height = min(rows, source.shape[0])
        tiles = source.shape[0] // height

        def one(i, carry):
            b = i // tiles
            r = pl.multiple_of(lax.rem(i, tiles) * height, height)
            cols = pl.ds(pl.multiple_of(b * W, W), W)
            out_rows = pl.ds(pl.multiple_of(base + r, height), height)
            level = inv[out_rows, :]
            lift = gain[gain.shape[0] - 1 :, cols] * (1.0 + mod_all[b, 2 + row : 3 + row, :])
            shift = mod_all[b, row : row + 1, :]
            x = source[pl.ds(r, height), cols].astype(F32)
            for h in range(H):
                c = slice(h * HEAD_DIM, (h + 1) * HEAD_DIM)
                to = pl.ds(pl.multiple_of(b * W + h * HEAD_DIM, HEAD_DIM), HEAD_DIM)
                hid[out_rows, to] = (x[:, c] * level * lift[:, c] + shift[:, c]).astype(BF16)
            return carry

        lax.fori_loop(0, tp_n * tiles, one, 0)

    modulate(ctx, T, 1)

    nt = min(256, W)

    def project(index, base, height):
        def one(j, carry):
            cols = pl.ds(pl.multiple_of(j * nt, nt), nt)
            product = dot(hid[base : base + height, :], wbuf[index, :, cols])
            proj[index, base : base + height, cols] = product.astype(BF16)
            return carry

        lax.fori_loop(0, W // nt, one, 0)

    loads[5].wait()
    loads[6].wait()
    project(1, T, CR)
    project(2, T, CR)

    scale = HEAD_DIM**-0.5
    step = token.astype(F32)
    low = (lane & 32) == 0
    cpos = (me * CR + lax.broadcasted_iota(jnp.int32, (CR, HEAD_DIM), 0)).astype(F32)
    ctotal = float(CR * sp_n)

    def put(ref, d, h, value):
        start = (d * H + h) * per
        ref[start : start + per] = value.reshape(per, R, HEAD_DIM).astype(BF16)

    for h in range(H):
        cols = slice(h * HEAD_DIM, (h + 1) * HEAD_DIM)
        ck = proj[1, T : T + CR, cols].astype(F32) * (scale * CONTEXT_LIFT)
        cv = proj[2, T : T + CR, cols]
        put(sc_send, 0, h, dot_rows((ck * jnp.exp(-fd[h] * (ctotal - 1.0 - cpos))).astype(BF16), cv))
        put(sc_send, 1, h, dot_rows((ck * jnp.exp(-bd[h] * cpos)).astype(BF16), cv))

    def scopy(off):
        return sp_copy(off, sc_send.at[lax.rem(me + off, sp_n)], sc_recv.at[me], scs, scr)

    def slcopy(off):
        return sp_copy(off, sl_send.at[lax.rem(me + off, sp_n)], sl_recv.at[me], sls, slr)

    def incopy(off):
        return sp_copy(off, in_send.at[lax.rem(me + off, sp_n)], in_recv.at[me], ins, inr)

    each(sp_n, lambda off: scopy(off).start())

    modulate(lat, 0, 0)
    project(1, 0, T)
    project(2, 0, T)

    for h in range(H):
        cols = slice(h * HEAD_DIM, (h + 1) * HEAD_DIM)
        k = rotated(proj[1, 0:T, cols].astype(F32), cosb[...], sinb[...], low) * scale
        v = proj[2, 0:T, cols]
        put(sl_send, 0, h, dot_rows((k * jnp.exp(-fd[h] * (T - 1.0 - step))).astype(BF16), v))
        put(sl_send, 1, h, dot_rows((k * jnp.exp(-bd[h] * step)).astype(BF16), v))
        proj[1, 0:T, cols] = k.astype(BF16)

    each(sp_n, lambda off: slcopy(off).start())
    relay(relay_y, 0)
    sc_recv[me] = sc_send[me]
    sl_recv[me] = sl_send[me]

    loads[7].wait()
    project(0, 0, T)
    loads[8].wait()
    project(3, 0, T)

    relay(relay_y, 1)
    each(sp_n, lambda off: scopy(off).wait_recv())
    each(sp_n, lambda off: slcopy(off).wait_recv())
    backward = (me * R) // (H * HEAD_DIM)
    head = lax.rem((me * R) // HEAD_DIM, H)
    rate = jnp.where(backward == 1, bd[head], fd[head])
    span = jnp.exp(jnp.full((R, HEAD_DIM), -float(T), F32) * rate)
    start = lax.fori_loop(
        0, sp_n, lambda s, total: total + sc_recv[s].astype(F32), jnp.zeros((R, HEAD_DIM), F32)
    )

    def scan(lap, state):
        i = jnp.where(backward == 1, sp_n - 1 - lap, lap)
        in_send[i] = state.astype(BF16)
        return span * state + sl_recv[i].astype(F32)

    lax.fori_loop(0, sp_n, scan, start)
    each(sp_n, lambda off: incopy(off).start())
    in_recv[me] = in_send[me]
    relay(relay_y, 2)

    st = 256 if T % 256 == 0 else mt
    for h in range(H):
        cols = slice(h * HEAD_DIM, (h + 1) * HEAD_DIM)
        q = rotated(proj[0, 0:T, cols].astype(F32), cosb[...], sinb[...], low).astype(BF16)
        proj[0, 0:T, cols] = q

        def score_rows(i, carry):
            r = pl.ds(pl.multiple_of(i * st, st), st)
            s = dot_columns(proj[0, r, cols], proj[1, 0:T, cols]) * mix[h, r, :].astype(F32)
            local[r, cols] = dot(s.astype(BF16), proj[2, 0:T, cols])
            return carry

        lax.fori_loop(0, T // st, score_rows, 0)

    relay(relay_y, 3)
    relay(relay_x, 0)
    each(sp_n, lambda off: incopy(off).wait_recv())

    def hview(block, h):
        return heads_all.at[block, :, pl.ds(h * HEAD_DIM, HEAD_DIM)]

    def hy(off, h):
        return remote(
            hview(tp, h), hview(tp, h), hys.at[off * H + h], hyr.at[off * H + h], y_peer(off)
        )

    def hp(off, h):
        block = y_source(off)
        return remote(
            hview(block, h),
            hview(block, h),
            hps.at[off * H + h],
            hpr.at[off * H + h],
            {"tp": other},
        )

    def hown(h):
        return remote(hview(tp, h), hview(tp, h), hps.at[h], hpr.at[h], {"tp": other})

    for h in range(H):
        cols = slice(h * HEAD_DIM, (h + 1) * HEAD_DIM)
        q = proj[0, 0:T, cols].astype(F32)
        at = h * per
        forward = in_recv[at : at + per].astype(F32).reshape(HEAD_DIM, HEAD_DIM).astype(BF16)
        at = (H + h) * per
        back = in_recv[at : at + per].astype(F32).reshape(HEAD_DIM, HEAD_DIM).astype(BF16)
        kept = (
            local[:, cols]
            + dot((q * jnp.exp(-fd[h] * (step + 1.0))).astype(BF16), forward)
            + dot((q * jnp.exp(-bd[h] * (T - step))).astype(BF16), back)
        )
        kept = kept * lax.rsqrt(jnp.mean(kept * kept, axis=-1, keepdims=True) + EPS)
        g = proj[3, 0:T, cols].astype(F32)
        heads_all[tp, :, cols] = (g / (1.0 + jnp.exp(-g)) * kept).astype(BF16)
        each(y_n, lambda off: hy(off, h).start())
        hown(h).start()

    relay(relay_x, 1)

    ot = min(256, W)

    def out_tile(j):
        cols = pl.ds(pl.multiple_of(j * ot, ot), ot)
        return pltpu.make_async_copy(out_v.at[:, cols], out_h.at[:, cols], out_sem.at[j])

    rows_each = HEAD_DIM * CN // W

    def product(blocks, low_head, high_head, first=False, last=False):
        k = slice(low_head * HEAD_DIM, high_head * HEAD_DIM)
        count = (high_head - low_head) * rows_each

        def one(j, carry):
            cols = pl.ds(pl.multiple_of(j * ot, ot), ot)
            value = None
            for block in blocks:
                chunk = pl.ds(block * CN + low_head * rows_each, count)
                weight = ow_all[chunk, :, cols].reshape((high_head - low_head) * HEAD_DIM, ot)
                term = dot(heads_all[block, :, k], weight)
                value = term if value is None else value + term
            if not first:
                value = value + acc[:, cols]
            if last:
                value = lat[:, cols].astype(F32) + gates[0:1, cols] * value
                out_v[:, cols] = value.astype(BF16)
                out_tile(j).start()
            else:
                acc[:, cols] = value
            return carry

        lax.fori_loop(0, D // ot, one, 0)

    loads[9].wait()
    for h in range(H):
        hown(h).wait_recv()
    wown.wait_recv()
    relay(relay_x, 2)
    product([tp, other], 0, H, first=True)
    relay(relay_x, 3)
    groups = [(0, H // 2), (H // 2, H)] if H > 1 else [(0, 1)]

    def far_step(off, group, last):
        low_head, high_head = groups[group]
        for h in range(low_head, high_head):
            hy(off, h).wait_recv()
            hp(off, h).start()
        for h in range(low_head, high_head):
            hp(off, h).wait_recv()
        if group == 0:
            for i in range(half):
                wp(off, i).wait_recv()
                wq(off, i).wait_recv()
        block = y_source(off)
        product([block, block + 1 - 2 * core], low_head, high_head, last=last)

    def middle(off):
        for group in range(len(groups)):
            far_step(off, group, False)

    each(y_n - 1, middle)
    for group in range(len(groups)):
        far_step(y_n - 1, group, group == len(groups) - 1)

    each(sp_n, lambda off: m1(off).wait_send())
    each(tp_n, lambda off: m2(off).wait_send())
    each(sp_n, lambda off: scopy(off).wait_send())
    each(sp_n, lambda off: slcopy(off).wait_send())
    each(sp_n, lambda off: incopy(off).wait_send())
    wown.wait_send()
    for h in range(H):
        hown(h).wait_send()

    def settle(off):
        for i in range(half):
            wy(off, i).wait_send()
            wx(off, i).wait_send()
            wp(off, i).wait_send()
            wq(off, i).wait_send()
        for h in range(H):
            hy(off, h).wait_send()
            hp(off, h).wait_send()

    each(y_n, settle)

    def written(j, carry):
        out_tile(j).wait()
        return carry

    lax.fori_loop(0, D // ot, written, 0)


def local_program(
    sp_n,
    tp_n,
    latent,
    context,
    condition,
    context_condition,
    shift_weight,
    scale_weight,
    mod_gate_weight,
    norm_gain,
    query_weight,
    key_weight,
    value_weight,
    gate_weight,
    forward_decay,
    backward_decay,
    out_weight,
):
    T, D = latent.shape
    CR = context.shape[0]
    MR, W = shift_weight.shape
    H = W // HEAD_DIM
    R = 2 * H * HEAD_DIM // sp_n
    CN = W // 64
    ow = out_weight.reshape(CN, W // CN, D)
    if MR % HEAD_DIM == 0:
        rows = jnp.concatenate([condition, context_condition, norm_gain])
        small = [rows.astype(F32).reshape(3, D)]
    else:
        pair = jnp.stack([condition, context_condition]).reshape(2, sp_n, MR)
        act = jnp.pad(jnp.transpose(pair, (1, 0, 2)), ((0, 0), (0, 14), (0, 0)))
        small = [norm_gain.astype(F32).reshape(1, D), act]
    y_n = tp_n // 2
    vm = pl.BlockSpec(memory_space=pltpu.VMEM)
    sm = pl.BlockSpec(memory_space=pltpu.SMEM)
    hb = pl.BlockSpec(memory_space=pl.ANY)
    V = pltpu.VMEM
    dma = pltpu.SemaphoreType.DMA
    state = V((sp_n, R, HEAD_DIM), BF16)
    return pl.pallas_call(
        functools.partial(kernel, sp_n, tp_n, len(small)),
        out_shape=jax.ShapeDtypeStruct((T, D), BF16),
        in_specs=[vm] * len(small) + [sm, sm] + [hb] * 10,
        out_specs=hb,
        scratch_shapes=[
            V((T, D), BF16),
            V((CR, D), BF16),
            V((3, MR, W), BF16),
            V((4, D, W), BF16),
            V((T + CR, D), BF16),
            V((8, W), F32),
            V((sp_n, 8, W), F32),
            V((8, W), F32),
            V((tp_n, 8, W), F32),
            V((T + CR, HEAD_DIM), F32),
            V((T, HEAD_DIM), F32),
            V((T, HEAD_DIM), F32),
            V((4, T + CR, W), BF16),
            V((H, T, T), BF16),
            V((T, W), F32),
            V((tp_n, T, W), BF16),
            V((tp_n * CN, W // CN, D), BF16),
            V((T, D), F32),
            V((8, D), F32),
            V((T, D), BF16),
            state,
            state,
            state,
            state,
            state,
            state,
            dma((10,)),
            dma((sp_n,)),
            dma((sp_n,)),
            dma((tp_n,)),
            dma((tp_n,)),
        ]
        + [dma((sp_n,))] * 6
        + [dma((1,))] * 2
        + [dma((y_n * CN // 2,))] * 8
        + [dma((y_n * H,))] * 4
        + [dma((D // min(256, W),))],
        compiler_params=pltpu.CompilerParams(
            collective_id=0, has_side_effects=True, vmem_limit_bytes=60 * 1024 * 1024
        ),
    )(
        *small,
        forward_decay,
        backward_decay,
        latent,
        context,
        shift_weight,
        scale_weight,
        mod_gate_weight,
        query_weight,
        key_weight,
        value_weight,
        gate_weight,
        ow,
    )


def solution(mesh):
    placed = (
        P("sp", None),
        P("sp", None),
        P(),
        P(),
        P("sp", "tp"),
        P("sp", "tp"),
        P("sp", "tp"),
        P(),
        P(None, "tp"),
        P(None, "tp"),
        P(None, "tp"),
        P(None, "tp"),
        P("tp"),
        P("tp"),
        P("tp", None),
    )
    return jax.shard_map(
        functools.partial(local_program, mesh.shape["sp"], mesh.shape["tp"]),
        mesh=mesh,
        in_specs=placed,
        out_specs=P("sp", None),
        check_vma=False,
    )
```

```python
import functools
import math

import jax
import jax.numpy as jnp
from jax import lax
from jax.experimental import pallas as pl
from jax.experimental.pallas import tpu as pltpu
from jax.sharding import PartitionSpec as P

HEAD_DIM = 128
GRID_W = 64
EPS = 1e-06
THETA = 10000.0
CONTEXT_LIFT = 3.0
MESH = pl.DeviceIdType.MESH
F32 = jnp.float32
BF16 = jnp.bfloat16


def dot(a, b):
    return jnp.dot(a, b, preferred_element_type=F32)


def dot_rows(a, b):
    return lax.dot_general(a, b, (((0,), (0,)), ((), ())), preferred_element_type=F32)


def dot_columns(a, b):
    return lax.dot_general(a, b, (((1,), (1,)), ((), ())), preferred_element_type=F32)


def rotated(x, cosines, sines, low):
    partner = jnp.where(low, pltpu.roll(x, HEAD_DIM - 32, 1), pltpu.roll(x, 32, 1))
    return x * cosines + partner * sines


def kernel(sp_n, tp_n, small_n, *refs):
    act = refs[1] if small_n == 2 else None
    body(sp_n, tp_n, act, refs[0], *refs[small_n:])


def body(
    sp_n,
    tp_n,
    act,
    gain,
    fd,
    bd,
    latent_h,
    context_h,
    shift_h,
    scale_h,
    gate_h,
    wq_h,
    wk_h,
    wv_h,
    wg_h,
    ow_h,
    out_h,
    lat,
    ctx,
    modw,
    wbuf,
    hid,
    mod_part,
    mod_recv,
    mod_sum,
    mod_all,
    inv,
    cosb,
    sinb,
    proj,
    mix,
    local,
    heads_all,
    ow_all,
    acc,
    gates,
    out_v,
    sc_send,
    sc_recv,
    sl_send,
    sl_recv,
    in_send,
    in_recv,
    load_sem,
    m1s,
    m1r,
    m2s,
    m2r,
    scs,
    scr,
    sls,
    slr,
    ins,
    inr,
    wos,
    wor,
    wys,
    wyr,
    wxs,
    wxr,
    wps,
    wpr,
    wqs,
    wqr,
    hys,
    hyr,
    hps,
    hpr,
    out_sem,
):
    me = lax.axis_index("sp")
    tp = lax.axis_index("tp")
    y_n = tp_n // 2
    my_y = tp // 2
    core = lax.rem(tp, 2)
    other = my_y * 2 + 1 - core
    T, D = lat.shape
    CR = ctx.shape[0]
    W = wbuf.shape[2]
    H = W // HEAD_DIM
    R = sl_send.shape[1]
    per = HEAD_DIM // R
    CN = ow_h.shape[0]
    half = CN // 2
    parity = lax.rem(me, 2)
    beside = me + 1 - 2 * parity

    loads = [
        pltpu.make_async_copy(src, dst, load_sem.at[i])
        for i, (src, dst) in enumerate(
            [
                (shift_h, modw.at[0]),
                (scale_h, modw.at[1]),
                (gate_h, modw.at[2]),
                (latent_h, lat),
                (context_h, ctx),
                (wk_h, wbuf.at[1]),
                (wv_h, wbuf.at[2]),
                (wq_h, wbuf.at[0]),
                (wg_h, wbuf.at[3]),
                (ow_h, ow_all.at[pl.ds(tp * CN, CN)]),
            ]
        )
    ]
    for load in loads:
        load.start()

    barrier = pltpu.get_barrier_semaphore()

    def greet(axis, mine, n):
        def one(off, carry):
            pl.semaphore_signal(
                barrier, inc=1, device_id={axis: lax.rem(mine + off, n)}, device_id_type=MESH
            )
            return carry

        lax.fori_loop(1, n, one, 0)

    greet("sp", me, sp_n)
    greet("tp", tp, tp_n)

    def remote(src, dst, ss, rs, where):
        return pltpu.make_async_remote_copy(
            src_ref=src,
            dst_ref=dst,
            send_sem=ss,
            recv_sem=rs,
            device_id=where,
            device_id_type=MESH,
        )

    def each(n, body):
        def one(off, carry):
            body(off)
            return carry

        lax.fori_loop(1, n, one, 0)

    def sp_copy(off, src, dst, ss, rs):
        return remote(src, dst, ss.at[off], rs.at[off], {"sp": lax.rem(me + off, sp_n)})

    MR = modw.shape[1]
    if act is None:
        a = gain[0:2, pl.ds(pl.multiple_of(me * MR, MR), MR)]
        a = jnp.concatenate([a, jnp.zeros((6, MR), F32)], axis=0)
    else:
        a = act[me].astype(F32)
    activation = (a / (1.0 + jnp.exp(-a))).astype(BF16)
    for i in range(3):
        loads[i].wait()
        mod_part[2 * i : 2 * i + 2, :] = dot(activation, modw[i])[0:2, :]
    mod_part[6:8, :] = jnp.zeros((2, W), F32)
    pl.semaphore_wait(barrier, sp_n - 1 + tp_n - 1)

    def m1(off):
        return sp_copy(off, mod_part, mod_recv.at[me], m1s, m1r)

    each(sp_n, lambda off: m1(off).start())

    def y_peer(off):
        return {"tp": lax.rem(my_y + off, y_n) * 2 + core}

    def y_source(off):
        return lax.rem(my_y - off + y_n, y_n) * 2 + core

    def wy(off, i):
        c = parity * half + i
        return remote(
            ow_h.at[c],
            ow_all.at[tp * CN + c],
            wys.at[off * half + i],
            wyr.at[off * half + i],
            y_peer(off),
        )

    each(y_n, lambda off: wy(off, 0).start())

    rows = 64
    loads[3].wait()
    loads[4].wait()

    def stat(source, base):
        height = min(rows, source.shape[0])

        def one(i, carry):
            r = pl.multiple_of(i * height, height)
            x = source[pl.ds(r, height), :].astype(F32)
            mean = jnp.mean(x * x, axis=-1, keepdims=True)
            inv[pl.ds(pl.multiple_of(base + r, height), height), :] = jnp.broadcast_to(
                lax.rsqrt(mean + EPS), (height, HEAD_DIM)
            )
            return carry

        lax.fori_loop(0, source.shape[0] // height, one, 0)

    stat(lat, 0)
    stat(ctx, T)

    each(sp_n, lambda off: m1(off).wait_recv())
    mod_recv[me] = mod_part[...]
    mod_sum[...] = lax.fori_loop(
        0, sp_n, lambda s, total: total + mod_recv[s], jnp.zeros((8, W), F32)
    )

    def m2(off):
        return remote(
            mod_sum,
            mod_all.at[tp],
            m2s.at[off],
            m2r.at[off],
            {"tp": lax.rem(tp + off, tp_n)},
        )

    each(tp_n, lambda off: m2(off).start())
    mod_all[tp] = mod_sum[...]

    token = lax.broadcasted_iota(jnp.int32, (T, HEAD_DIM), 0)
    lane = lax.broadcasted_iota(jnp.int32, (T, HEAD_DIM), 1)
    place = me * T + token
    spot = jnp.where(lane < 64, place >> 6, place & 63).astype(F32)
    angle = spot * jnp.exp((lane & 31).astype(F32) * (-math.log(THETA) / 32.0))
    cosb[...] = jnp.cos(angle)
    sine = jnp.sin(angle)
    sinb[...] = jnp.where((lane & 32) == 0, -sine, sine)

    mt = 128

    def mix_rows(i, carry):
        r = pl.multiple_of(i * mt, mt)
        gap = (
            i * mt
            + lax.broadcasted_iota(jnp.int32, (mt, T), 0)
            - lax.broadcasted_iota(jnp.int32, (mt, T), 1)
        )
        gapf = gap.astype(F32)
        for h in range(H):
            weight = jnp.exp(jnp.where(gap >= 0, -fd[h] * gapf, bd[h] * gapf))
            mix[h, pl.ds(r, mt), :] = jnp.where(gap == 0, 2.0, weight).astype(BF16)
        return carry

    lax.fori_loop(0, T // mt, mix_rows, 0)

    each(tp_n, lambda off: m2(off).wait_recv())

    def gate_row(b, carry):
        gates[0:1, pl.ds(pl.multiple_of(b * W, W), W)] = mod_all[b, 4:5, :]
        return carry

    lax.fori_loop(0, tp_n, gate_row, 0)

    wown = remote(ow_h, ow_all.at[pl.ds(tp * CN, CN)], wos.at[0], wor.at[0], {"tp": other})

    def passed(off, i, side, ss, rs, where):
        c = ow_all.at[y_source(off) * CN + side * half + i]
        return remote(c, c, ss.at[off * half + i], rs.at[off * half + i], where)

    def wx(off, i):
        return passed(off, i, parity, wxs, wxr, {"sp": beside})

    def wp(off, i):
        return passed(off, i, parity, wps, wpr, {"tp": other})

    def wq(off, i):
        return passed(off, i, 1 - parity, wqs, wqr, {"tp": other})

    for i in range(1, half):
        each(y_n, lambda off: wy(off, i).start())
    wown.start()

    def relay_y(i):
        def one(off):
            wy(off, i).wait_recv()
            wx(off, i).start()
            wp(off, i).start()

        each(y_n, one)

    def relay_x(i):
        def one(off):
            wx(off, i).wait_recv()
            wq(off, i).start()

        each(y_n, one)

    quarter = max(half // 4, 1)

    def relay(which, phase):
        for i in range(phase * quarter, min((phase + 1) * quarter, half)):
            which(i)

    def modulate(source, base, row):
        height = min(rows, source.shape[0])
        tiles = source.shape[0] // height

        def one(i, carry):
            b = i // tiles
            r = pl.multiple_of(lax.rem(i, tiles) * height, height)
            cols = pl.ds(pl.multiple_of(b * W, W), W)
            out_rows = pl.ds(pl.multiple_of(base + r, height), height)
            level = inv[out_rows, :]
            lift = gain[gain.shape[0] - 1 :, cols] * (1.0 + mod_all[b, 2 + row : 3 + row, :])
            shift = mod_all[b, row : row + 1, :]
            x = source[pl.ds(r, height), cols].astype(F32)
            for h in range(H):
                c = slice(h * HEAD_DIM, (h + 1) * HEAD_DIM)
                to = pl.ds(pl.multiple_of(b * W + h * HEAD_DIM, HEAD_DIM), HEAD_DIM)
                hid[out_rows, to] = (x[:, c] * level * lift[:, c] + shift[:, c]).astype(BF16)
            return carry

        lax.fori_loop(0, tp_n * tiles, one, 0)

    relay(relay_y, 0)
    modulate(ctx, T, 1)

    nt = min(256, W)

    def project(index, base, height):
        def one(j, carry):
            cols = pl.ds(pl.multiple_of(j * nt, nt), nt)
            product = dot(hid[base : base + height, :], wbuf[index, :, cols])
            proj[index, base : base + height, cols] = product.astype(BF16)
            return carry

        lax.fori_loop(0, W // nt, one, 0)

    loads[5].wait()
    loads[6].wait()
    project(1, T, CR)
    project(2, T, CR)

    scale = HEAD_DIM**-0.5
    step = token.astype(F32)
    low = (lane & 32) == 0
    cpos = (me * CR + lax.broadcasted_iota(jnp.int32, (CR, HEAD_DIM), 0)).astype(F32)
    ctotal = float(CR * sp_n)

    def put(ref, d, h, value):
        start = (d * H + h) * per
        ref[start : start + per] = value.reshape(per, R, HEAD_DIM).astype(BF16)

    for h in range(H):
        cols = slice(h * HEAD_DIM, (h + 1) * HEAD_DIM)
        ck = proj[1, T : T + CR, cols].astype(F32) * (scale * CONTEXT_LIFT)
        cv = proj[2, T : T + CR, cols]
        put(sc_send, 0, h, dot_rows((ck * jnp.exp(-fd[h] * (ctotal - 1.0 - cpos))).astype(BF16), cv))
        put(sc_send, 1, h, dot_rows((ck * jnp.exp(-bd[h] * cpos)).astype(BF16), cv))

    def scopy(off):
        return sp_copy(off, sc_send.at[lax.rem(me + off, sp_n)], sc_recv.at[me], scs, scr)

    def slcopy(off):
        return sp_copy(off, sl_send.at[lax.rem(me + off, sp_n)], sl_recv.at[me], sls, slr)

    def incopy(off):
        return sp_copy(off, in_send.at[lax.rem(me + off, sp_n)], in_recv.at[me], ins, inr)

    each(sp_n, lambda off: scopy(off).start())

    modulate(lat, 0, 0)
    project(1, 0, T)
    project(2, 0, T)

    for h in range(H):
        cols = slice(h * HEAD_DIM, (h + 1) * HEAD_DIM)
        k = rotated(proj[1, 0:T, cols].astype(F32), cosb[...], sinb[...], low) * scale
        v = proj[2, 0:T, cols]
        put(sl_send, 0, h, dot_rows((k * jnp.exp(-fd[h] * (T - 1.0 - step))).astype(BF16), v))
        put(sl_send, 1, h, dot_rows((k * jnp.exp(-bd[h] * step)).astype(BF16), v))
        proj[1, 0:T, cols] = k.astype(BF16)

    each(sp_n, lambda off: slcopy(off).start())
    relay(relay_y, 1)
    sc_recv[me] = sc_send[me]
    sl_recv[me] = sl_send[me]

    loads[7].wait()
    project(0, 0, T)
    loads[8].wait()
    project(3, 0, T)

    each(sp_n, lambda off: scopy(off).wait_recv())
    each(sp_n, lambda off: slcopy(off).wait_recv())
    backward = (me * R) // (H * HEAD_DIM)
    head = lax.rem((me * R) // HEAD_DIM, H)
    rate = jnp.where(backward == 1, bd[head], fd[head])
    span = jnp.exp(jnp.full((R, HEAD_DIM), -float(T), F32) * rate)
    start = lax.fori_loop(
        0, sp_n, lambda s, total: total + sc_recv[s].astype(F32), jnp.zeros((R, HEAD_DIM), F32)
    )

    def scan(lap, state):
        i = jnp.where(backward == 1, sp_n - 1 - lap, lap)
        in_send[i] = state.astype(BF16)
        return span * state + sl_recv[i].astype(F32)

    lax.fori_loop(0, sp_n, scan, start)
    each(sp_n, lambda off: incopy(off).start())
    in_recv[me] = in_send[me]
    relay(relay_y, 2)

    st = 256 if T % 256 == 0 else mt
    for h in range(H):
        cols = slice(h * HEAD_DIM, (h + 1) * HEAD_DIM)
        q = rotated(proj[0, 0:T, cols].astype(F32), cosb[...], sinb[...], low).astype(BF16)
        proj[0, 0:T, cols] = q

        def score_rows(i, carry):
            r = pl.ds(pl.multiple_of(i * st, st), st)
            s = dot_columns(proj[0, r, cols], proj[1, 0:T, cols]) * mix[h, r, :].astype(F32)
            local[r, cols] = dot(s.astype(BF16), proj[2, 0:T, cols])
            return carry

        lax.fori_loop(0, T // st, score_rows, 0)

    relay(relay_y, 3)
    relay(relay_x, 0)
    each(sp_n, lambda off: incopy(off).wait_recv())

    def hview(block, h):
        return heads_all.at[block, :, pl.ds(h * HEAD_DIM, HEAD_DIM)]

    def hy(off, h):
        return remote(
            hview(tp, h), hview(tp, h), hys.at[off * H + h], hyr.at[off * H + h], y_peer(off)
        )

    def hp(off, h):
        block = y_source(off)
        return remote(
            hview(block, h),
            hview(block, h),
            hps.at[off * H + h],
            hpr.at[off * H + h],
            {"tp": other},
        )

    def hown(h):
        return remote(hview(tp, h), hview(tp, h), hps.at[h], hpr.at[h], {"tp": other})

    for h in range(H):
        cols = slice(h * HEAD_DIM, (h + 1) * HEAD_DIM)
        q = proj[0, 0:T, cols].astype(F32)
        at = h * per
        forward = in_recv[at : at + per].astype(F32).reshape(HEAD_DIM, HEAD_DIM).astype(BF16)
        at = (H + h) * per
        back = in_recv[at : at + per].astype(F32).reshape(HEAD_DIM, HEAD_DIM).astype(BF16)
        kept = (
            local[:, cols]
            + dot((q * jnp.exp(-fd[h] * (step + 1.0))).astype(BF16), forward)
            + dot((q * jnp.exp(-bd[h] * (T - step))).astype(BF16), back)
        )
        kept = kept * lax.rsqrt(jnp.mean(kept * kept, axis=-1, keepdims=True) + EPS)
        g = proj[3, 0:T, cols].astype(F32)
        heads_all[tp, :, cols] = (g / (1.0 + jnp.exp(-g)) * kept).astype(BF16)
        each(y_n, lambda off: hy(off, h).start())
        hown(h).start()

    relay(relay_x, 1)

    ot = min(256, W)

    def out_tile(j):
        cols = pl.ds(pl.multiple_of(j * ot, ot), ot)
        return pltpu.make_async_copy(out_v.at[:, cols], out_h.at[:, cols], out_sem.at[j])

    rows_each = HEAD_DIM * CN // W

    def product(blocks, low_head, high_head, first=False, last=False):
        k = slice(low_head * HEAD_DIM, high_head * HEAD_DIM)
        count = (high_head - low_head) * rows_each

        def one(j, carry):
            cols = pl.ds(pl.multiple_of(j * ot, ot), ot)
            value = None
            for block in blocks:
                chunk = pl.ds(block * CN + low_head * rows_each, count)
                weight = ow_all[chunk, :, cols].reshape((high_head - low_head) * HEAD_DIM, ot)
                term = dot(heads_all[block, :, k], weight)
                value = term if value is None else value + term
            if not first:
                value = value + acc[:, cols]
            if last:
                value = lat[:, cols].astype(F32) + gates[0:1, cols] * value
                out_v[:, cols] = value.astype(BF16)
                out_tile(j).start()
            else:
                acc[:, cols] = value
            return carry

        lax.fori_loop(0, D // ot, one, 0)

    loads[9].wait()
    for h in range(H):
        hown(h).wait_recv()
    wown.wait_recv()
    relay(relay_x, 2)
    product([tp, other], 0, H, first=True)
    relay(relay_x, 3)
    groups = [(0, H // 2), (H // 2, H)] if H > 1 else [(0, 1)]

    def far_step(off, group, last):
        low_head, high_head = groups[group]
        for h in range(low_head, high_head):
            hy(off, h).wait_recv()
            hp(off, h).start()
        for h in range(low_head, high_head):
            hp(off, h).wait_recv()
        if group == 0:
            for i in range(half):
                wp(off, i).wait_recv()
                wq(off, i).wait_recv()
        block = y_source(off)
        product([block, block + 1 - 2 * core], low_head, high_head, last=last)

    def middle(off):
        for group in range(len(groups)):
            far_step(off, group, False)

    each(y_n - 1, middle)
    for group in range(len(groups)):
        far_step(y_n - 1, group, group == len(groups) - 1)

    each(sp_n, lambda off: m1(off).wait_send())
    each(tp_n, lambda off: m2(off).wait_send())
    each(sp_n, lambda off: scopy(off).wait_send())
    each(sp_n, lambda off: slcopy(off).wait_send())
    each(sp_n, lambda off: incopy(off).wait_send())
    wown.wait_send()
    for h in range(H):
        hown(h).wait_send()

    def settle(off):
        for i in range(half):
            wy(off, i).wait_send()
            wx(off, i).wait_send()
            wp(off, i).wait_send()
            wq(off, i).wait_send()
        for h in range(H):
            hy(off, h).wait_send()
            hp(off, h).wait_send()

    each(y_n, settle)

    def written(j, carry):
        out_tile(j).wait()
        return carry

    lax.fori_loop(0, D // ot, written, 0)


def local_program(
    sp_n,
    tp_n,
    latent,
    context,
    condition,
    context_condition,
    shift_weight,
    scale_weight,
    mod_gate_weight,
    norm_gain,
    query_weight,
    key_weight,
    value_weight,
    gate_weight,
    forward_decay,
    backward_decay,
    out_weight,
):
    T, D = latent.shape
    CR = context.shape[0]
    MR, W = shift_weight.shape
    H = W // HEAD_DIM
    R = 2 * H * HEAD_DIM // sp_n
    CN = W // 64
    ow = out_weight.reshape(CN, W // CN, D)
    if MR % HEAD_DIM == 0:
        rows = jnp.concatenate([condition, context_condition, norm_gain])
        small = [rows.astype(F32).reshape(3, D)]
    else:
        pair = jnp.stack([condition, context_condition]).reshape(2, sp_n, MR)
        act = jnp.pad(jnp.transpose(pair, (1, 0, 2)), ((0, 0), (0, 14), (0, 0)))
        small = [norm_gain.astype(F32).reshape(1, D), act]
    y_n = tp_n // 2
    vm = pl.BlockSpec(memory_space=pltpu.VMEM)
    sm = pl.BlockSpec(memory_space=pltpu.SMEM)
    hb = pl.BlockSpec(memory_space=pl.ANY)
    V = pltpu.VMEM
    dma = pltpu.SemaphoreType.DMA
    state = V((sp_n, R, HEAD_DIM), BF16)
    return pl.pallas_call(
        functools.partial(kernel, sp_n, tp_n, len(small)),
        out_shape=jax.ShapeDtypeStruct((T, D), BF16),
        in_specs=[vm] * len(small) + [sm, sm] + [hb] * 10,
        out_specs=hb,
        scratch_shapes=[
            V((T, D), BF16),
            V((CR, D), BF16),
            V((3, MR, W), BF16),
            V((4, D, W), BF16),
            V((T + CR, D), BF16),
            V((8, W), F32),
            V((sp_n, 8, W), F32),
            V((8, W), F32),
            V((tp_n, 8, W), F32),
            V((T + CR, HEAD_DIM), F32),
            V((T, HEAD_DIM), F32),
            V((T, HEAD_DIM), F32),
            V((4, T + CR, W), BF16),
            V((H, T, T), BF16),
            V((T, W), F32),
            V((tp_n, T, W), BF16),
            V((tp_n * CN, W // CN, D), BF16),
            V((T, D), F32),
            V((8, D), F32),
            V((T, D), BF16),
            state,
            state,
            state,
            state,
            state,
            state,
            dma((10,)),
            dma((sp_n,)),
            dma((sp_n,)),
            dma((tp_n,)),
            dma((tp_n,)),
        ]
        + [dma((sp_n,))] * 6
        + [dma((1,))] * 2
        + [dma((y_n * CN // 2,))] * 8
        + [dma((y_n * H,))] * 4
        + [dma((D // min(256, W),))],
        compiler_params=pltpu.CompilerParams(
            collective_id=0, has_side_effects=True, vmem_limit_bytes=60 * 1024 * 1024
        ),
    )(
        *small,
        forward_decay,
        backward_decay,
        latent,
        context,
        shift_weight,
        scale_weight,
        mod_gate_weight,
        query_weight,
        key_weight,
        value_weight,
        gate_weight,
        ow,
    )


def solution(mesh):
    placed = (
        P("sp", None),
        P("sp", None),
        P(),
        P(),
        P("sp", "tp"),
        P("sp", "tp"),
        P("sp", "tp"),
        P(),
        P(None, "tp"),
        P(None, "tp"),
        P(None, "tp"),
        P(None, "tp"),
        P("tp"),
        P("tp"),
        P("tp", None),
    )
    return jax.shard_map(
        functools.partial(local_program, mesh.shape["sp"], mesh.shape["tp"]),
        mesh=mesh,
        in_specs=placed,
        out_specs=P("sp", None),
        check_vma=False,
    )
```
